256 devices in a mesh: rep: 2 (over z_hi), fs: 16 (over z_lo, x), tp: 8 (over y, core).
Axes of the slice: x: 4, y: 4, z: 8 (z_hi: 2, z_lo: 4; z = z_hi * 4 + z_lo), core: 2. Of those that a mesh axis runs over, the one named last changes fastest.
Arguments:
- tokens: bfloat16 [24576, 2048], P(('rep', 'fs'), 'tp'), parts along dimension 0, may hold values from -6 to 6
- mixer_gain: float32 [2048], replicated, may hold values from 0.1 to 1.9
- rec_weight: bfloat16 [2048, 2048], P('fs', 'tp'), may hold values from -0.125 to 0.125
- gate_weight: bfloat16 [2048, 2048], P('fs', 'tp'), may hold values from -0.125 to 0.125
- conv_taps: bfloat16 [4, 2048], P(None, 'tp'), may hold values from -3 to 3
- recur_map: bfloat16 [8, 256, 256], P('tp'), may hold values from -0.375 to 0.375
- input_map: bfloat16 [8, 256, 256], P('tp'), may hold values from -0.375 to 0.375
- decay_param: float32 [2048], P('tp'), may hold values from 3 to 11
- out_weight: bfloat16 [2048, 2048], P('tp', 'fs'), may hold values from -0.5 to 0.5
- mlp_gain: float32 [2048], replicated, may hold values from 0.1 to 1.9
- up_weight: bfloat16 [2048, 8192], P('fs', 'tp'), may hold values from -0.125 to 0.125
- down_weight: bfloat16 [8192, 2048], P('tp', 'fs'), may hold values from -0.0625 to 0.0625
Outputs:
- layer_out: bfloat16 [24576, 2048], P(('rep', 'fs'), 'tp'), parts along dimension 0
The draws below stay inside these ranges and needn't reach their ends.
There are 2 independent parts, one for each index of `rep`. The reference program is written for one: setup_inputs(seed, part) draws one part's arguments, and reference() takes and returns one part's arrays. A program takes and returns all parts, laid end to end along the dimension named above; an argument that names none is the same for every part. Nothing has to cross between parts.
All inputs are finite; a program needn't handle non-finite values.
Results may differ from the reference program's by a relative error of at most 0.022.
Values may be sent and summed in bfloat16 or wider, within the bound.
A program may use at most 64 MiB of HBM per device.

```python
import math
import jax
import jax.numpy as jnp
from jax import lax

D = 2048
D_RNN = 2048
FF = 8192
N_BLOCKS = 8
CONV_W = 4
TOK_DEV = 768
TOKENS = 12288
BLOCK_W = 256
CH_DEV = 256
FF_DEV = 1024


def draw_decay_param(key, part):
    mask_key, slow_key, quick_key = jax.random.split(jax.random.fold_in(key, 17), 3)
    quick_share = 0.5
    is_quick = jax.random.bernoulli(mask_key, quick_share, (D_RNN,))
    slow_rate = jnp.exp(jax.random.uniform(slow_key, (D_RNN,), jnp.float32, math.log(0.05 / TOK_DEV), math.log(0.4 / TOK_DEV)))
    quick_rate = jnp.exp(jax.random.uniform(quick_key, (D_RNN,), jnp.float32, math.log(0.0025), math.log(0.008)))
    chosen_rate = jnp.where(is_quick, quick_rate, slow_rate)
    return (-jnp.log(jnp.expm1(chosen_rate))).astype(jnp.float32)


def level_of(rng, dims, cuts, low, high):
    loudness, own = 1.0, jax.random.fold_in(rng, 6)
    for dim, shards_of in cuts:
        draws = jnp.exp(jax.random.uniform(jax.random.fold_in(own, dim), (shards_of,), jnp.float32, low / len(cuts), high / len(cuts)))
        loudness = loudness * jnp.repeat(draws, dims[dim] // shards_of).reshape([-1 if axis == dim else 1 for axis in range(len(dims))])
    return loudness


def scatter_about(own_key, shape, spread, most, cuts=(), held_as=jnp.bfloat16):
    drawn = spread * jax.random.normal(own_key, shape, jnp.float32)
    if cuts:
        drawn = drawn * level_of(own_key, shape, cuts, -0.22, 0.18)
    return jnp.clip(drawn, -most, most).astype(held_as)


def setup_inputs(seed: int = 0, part: int = 0) -> dict:
    key_of = jax.random.split(jax.random.key(seed), 13)
    part_keys = jax.random.split(jax.random.fold_in(key_of[12], part), 13)
    tokens = scatter_about(part_keys[0], (TOKENS, D), 1.0, 6.0, ((0, 16), (1, 8)))
    mixer_gain = jnp.clip(1.0 + 0.18 * jax.random.normal(key_of[1], (D,), jnp.float32), 0.1, 1.9)
    rec_weight = scatter_about(key_of[2], (D, D_RNN), D ** -0.5, 0.125, ((0, 16), (1, 8)))
    gate_weight = scatter_about(key_of[3], (D, D_RNN), D ** -0.5, 0.125, ((0, 16), (1, 8)))
    conv_taps = scatter_about(key_of[4], (CONV_W, D_RNN), CONV_W ** -0.5, 3.0, ((1, 8),))
    recur_map = scatter_about(key_of[5], (N_BLOCKS, BLOCK_W, BLOCK_W), BLOCK_W ** -0.5, 0.375, ((0, 8),))
    input_map = scatter_about(key_of[6], (N_BLOCKS, BLOCK_W, BLOCK_W), BLOCK_W ** -0.5, 0.375, ((0, 8),))
    decay_param = draw_decay_param(jax.random.fold_in(key_of[12], 71), part)
    out_weight = scatter_about(key_of[8], (D_RNN, D), (D_RNN // 16) ** -0.5, 0.5, ((0, 8), (1, 16)))
    mlp_gain = jnp.clip(1.0 + 0.18 * jax.random.normal(key_of[9], (D,), jnp.float32), 0.1, 1.9)
    up_weight = scatter_about(key_of[10], (D, FF), D ** -0.5, 0.125, ((0, 16), (1, 8)))
    down_weight = scatter_about(key_of[11], (FF, D), FF ** -0.5, 0.0625, ((0, 8), (1, 16)))
    return {"tokens": tokens, "mixer_gain": mixer_gain, "rec_weight": rec_weight, "gate_weight": gate_weight, "conv_taps": conv_taps, "recur_map": recur_map, "input_map": input_map, "decay_param": decay_param, "out_weight": out_weight, "mlp_gain": mlp_gain, "up_weight": up_weight, "down_weight": down_weight}


NORM_EPSILON = 1e-06
GATE_SCALE = 8.0

def rms_rows(full_rows, gain):
    widened = full_rows.astype(jnp.float32)
    inverse = lax.rsqrt(lax.optimization_barrier(jnp.mean(widened * widened, axis=-1, keepdims=True)) + NORM_EPSILON)
    return (widened * inverse * gain.astype(jnp.float32)).astype(jnp.bfloat16)

def causal_taps(branch, conv_taps):
    widened = branch.astype(jnp.float32)
    tap_values = conv_taps.astype(jnp.float32)
    tap_count = tap_values.shape[0]
    length = widened.shape[-2]
    padded = jnp.pad(widened, [(0, 0)] * (widened.ndim - 2) + [(tap_count - 1, 0), (0, 0)])
    running = jnp.zeros_like(widened)
    for offset in range(tap_count):
        running = running + padded[..., offset:offset + length, :] * tap_values[offset]
    return running.astype(jnp.bfloat16)

def combine(earlier, latter):
    return (earlier[0] * latter[0], latter[0] * earlier[1] + latter[1])

def blocked_sum(hidden, weight, block):
    running = jnp.zeros((hidden.shape[0], weight.shape[1]), jnp.float32)
    for offset in range(0, hidden.shape[1], block):
        partial_value = jnp.dot(hidden[:, offset:offset + block], weight[offset:offset + block], preferred_element_type=jnp.float32)
        rounded = lax.optimization_barrier(partial_value.astype(jnp.bfloat16))
        running = running + rounded.astype(jnp.float32)
    return running

def reference(tokens, mixer_gain, rec_weight, gate_weight, conv_taps, recur_map, input_map, decay_param, out_weight, mlp_gain, up_weight, down_weight):
    normed = rms_rows(tokens, mixer_gain)
    branch = jnp.dot(normed, rec_weight, preferred_element_type=jnp.float32).astype(jnp.bfloat16)
    gate_branch = jnp.dot(normed, gate_weight, preferred_element_type=jnp.float32).astype(jnp.bfloat16)
    seq_count = tokens.shape[0] // TOK_DEV
    conv_out = causal_taps(branch.reshape(seq_count, TOK_DEV, D_RNN), conv_taps)
    blocks = conv_out.astype(jnp.float32).reshape(seq_count, TOK_DEV, N_BLOCKS, BLOCK_W)
    recur_gate = jax.nn.sigmoid(jnp.einsum('slnc,ncd->slnd', blocks, recur_map.astype(jnp.float32)).reshape(seq_count, TOK_DEV, D_RNN))
    input_gate = jax.nn.sigmoid(jnp.einsum('slnc,ncd->slnd', blocks, input_map.astype(jnp.float32)).reshape(seq_count, TOK_DEV, D_RNN))
    log_decay = -GATE_SCALE * recur_gate * jax.nn.softplus(-decay_param.astype(jnp.float32))
    decay_rate = jnp.exp(log_decay)
    drive_term = jnp.sqrt(-jnp.expm1(2.0 * log_decay)) * (input_gate * conv_out.astype(jnp.float32))
    _, states = lax.associative_scan(combine, (decay_rate, drive_term), axis=1)
    gate_act = jax.nn.gelu(gate_branch.astype(jnp.float32)).reshape(seq_count, TOK_DEV, D_RNN)
    mixed_out = (states * gate_act).astype(jnp.bfloat16)
    mixed_out = mixed_out.reshape(seq_count * TOK_DEV, D_RNN)
    mixer_out = blocked_sum(mixed_out, out_weight, CH_DEV)
    middle = (tokens.astype(jnp.float32) + mixer_out).astype(jnp.bfloat16)
    normed_mlp = rms_rows(middle, mlp_gain)
    lifted = jnp.dot(normed_mlp, up_weight, preferred_element_type=jnp.float32)
    squared = jnp.square(jax.nn.relu(lifted)).astype(jnp.bfloat16)
    mlp_out = blocked_sum(squared, down_weight, FF_DEV)
    return (middle.astype(jnp.float32) + mlp_out).astype(jnp.bfloat16)
```

```python
import jax
import jax.numpy as jnp
from jax import lax
from jax.experimental import pallas as pl
from jax.experimental.pallas import tpu as pltpu
from jax.sharding import PartitionSpec as P

NORM_EPSILON = 1e-06
GATE_SCALE = 8.0
MESH = pl.DeviceIdType.MESH
F32 = jnp.float32
BF16 = jnp.bfloat16

TOK = 768
D = 2048
CH = 256
FF = 1024
CHUNKS = 4
R = TOK // CHUNKS
H = R // 2
SEGS = 8
SEG = TOK // SEGS


def send(src, dst, send_sem, recv_sem, device):
    pltpu.make_async_remote_copy(
        src_ref=src,
        dst_ref=dst,
        send_sem=send_sem,
        recv_sem=recv_sem,
        device_id=device,
        device_id_type=MESH,
    ).start()


def landed(ref, sem):
    pltpu.make_async_copy(ref, ref, sem).wait()


def minus_expm1(u):
    series = 1.0 + u * (1.0 / 8.0)
    for k in (7.0, 6.0, 5.0, 4.0, 3.0, 2.0):
        series = 1.0 + (u * (1.0 / k)) * series
    return jnp.where(u > -0.5, -u * series, 1.0 - jnp.exp(u))


def kernel(
    tokens,
    rec_shard,
    gate_shard,
    out_shard,
    up_shard,
    down_shard,
    mixer_gain,
    conv_taps,
    recur_map,
    input_map,
    decay_param,
    mlp_gain,
    result,
    w_rec,
    w_gate,
    w_out,
    w_up,
    w_down,
    tok_all,
    mid_all,
    normed,
    padded,
    gate_act,
    decay,
    drive,
    mixed,
    squared,
    part_out,
    part_own,
    from_core,
    half_sent,
    half_got,
    full_sent,
    full_got,
    local_sem,
    w_sem,
    ag_sem,
    rs_sem,
):
    rep, fs, tp = lax.axis_index("rep"), lax.axis_index("fs"), lax.axis_index("tp")
    z, x = lax.div(fs, 4), lax.rem(fs, 4)
    y, core = lax.div(tp, 2), lax.rem(tp, 2)
    other = 1 - core
    xp, xm, x2 = lax.rem(x + 1, 4), lax.rem(x + 3, 4), lax.rem(x + 2, 4)
    zp, zm, z2 = lax.rem(z + 1, 4), lax.rem(z + 3, 4), lax.rem(z + 2, 4)
    yp, ym, y2 = lax.rem(y + 1, 4), lax.rem(y + 3, 4), lax.rem(y + 2, 4)
    deep = rep * 4 + z
    deep_p, deep_m = lax.rem(deep + 1, 8), lax.rem(deep + 7, 8)
    x_up, x_down = (rep, z * 4 + xp, tp), (rep, z * 4 + xm, tp)
    z_up = (lax.div(deep_p, 4), zp * 4 + x, tp)
    z_down = (lax.div(deep_m, 4), zm * 4 + x, tp)
    y_up, y_down = (rep, fs, yp * 2 + core), (rep, fs, ym * 2 + core)
    partner = (rep, fs, y * 2 + other)

    places = (
        (tokens, tok_all.at[tp]),
        (rec_shard, w_rec.at[z, x]),
        (gate_shard, w_gate.at[z, x]),
        (out_shard, w_out.at[z, x]),
        (up_shard, w_up.at[z, x]),
        (down_shard, w_down.at[z, x]),
    )
    fills = [pltpu.make_async_copy(s, d, local_sem.at[k]) for k, (s, d) in enumerate(places)]
    for fill in fills:
        fill.start()
    barrier = pltpu.get_barrier_semaphore()
    for device in (x_up, x_down, z_up, z_down, y_up, y_down, partner):
        pl.semaphore_signal(barrier, inc=1, device_id=device, device_id_type=MESH)
    pl.semaphore_wait(barrier, 7)
    for fill in fills:
        fill.wait()

    def copies(k, w, recv, sent, *moves):
        for index, device in moves:
            ref = w.at[index]
            send(ref, ref, w_sem.at[k, sent], w_sem.at[k, recv], device)

    weights = {"rec": (0, w_rec), "gate": (1, w_gate), "out": (2, w_out), "up": (3, w_up), "down": (4, w_down)}

    def pieces(w):
        h = w.shape[2] // 2
        q = h // 2
        return pl.ds(0, h), pl.ds(h, h), pl.ds(0, q), pl.ds(q, q), pl.ds(h, q), pl.ds(h + q, q)

    def w1(name):
        k, w = weights[name]
        a, b, _, _, _, _ = pieces(w)
        copies(k, w, 0, 4, ((z, x, a), x_up), ((z, x, a), x_down), ((z, x, b), z_up), ((z, x, b), z_down))
        copies(k, w, 2, 4, ((z, x, a), z_up), ((z, x, a), z_down), ((z, x, b), x_up), ((z, x, b), x_down))

    def w2(name):
        k, w = weights[name]
        a, b, at, ab, bt, bb = pieces(w)
        landed(w.at[0, pl.ds(0, 2)], w_sem.at[k, 0])
        copies(k, w, 1, 5, ((z, xm, at), x_up), ((z, xp, ab), x_down), ((zm, x, bt), z_up), ((zp, x, bb), z_down))
        for n in (xm, xp):
            copies(k, w, 2, 4, ((z, n, a), z_up), ((z, n, a), z_down))
        for n in (zm, zp):
            copies(k, w, 2, 4, ((n, x, b), x_up), ((n, x, b), x_down))

    def w3(name):
        k, w = weights[name]
        a, b, _, _, _, _ = pieces(w)
        landed(w.at[0, 0], w_sem.at[k, 1])
        copies(k, w, 2, 5, ((z, x2, a), z_up), ((z, x2, a), z_down), ((z2, x, b), x_up), ((z2, x, b), x_down))

    def w4(name):
        k, w = weights[name]
        every = pl.ds(0, 4)
        _, _, at, ab, bt, bb = pieces(w)
        landed(w.at[pl.ds(0, 2)], w_sem.at[k, 2])
        copies(k, w, 3, 6, ((zm, every, at), z_up), ((zp, every, ab), z_down), ((every, xm, bt), x_up), ((every, xp, bb), x_down))

    def w5(name):
        k, w = weights[name]
        landed(w.at[0], w_sem.at[k, 3])

    def w_drain():
        for k, w in weights.values():
            landed(w.at[pl.ds(0, 2)], w_sem.at[k, 4])
            landed(w.at[0, pl.ds(0, 3)], w_sem.at[k, 5])
            landed(w.at[0], w_sem.at[k, 6])

    jp, jm, j2 = yp * 2 + core, ym * 2 + core, y2 * 2 + core

    def ag(k, buf, first, count):
        rows, top, bottom = pl.ds(first, count), pl.ds(first, count // 2), pl.ds(first + count // 2, count // 2)
        sem = lambda n: ag_sem.at[k, n]
        move = lambda index, recv, device: send(buf.at[index], buf.at[index], sem(3), sem(recv), device)

        def one():
            move((tp, rows), 0, y_up)
            move((tp, rows), 0, y_down)
            move((tp, rows), 2, partner)

        def two():
            landed(buf.at[pl.ds(0, 2), rows], sem(0))
            move((jm, top), 1, y_up)
            move((jp, bottom), 1, y_down)
            move((jm, rows), 2, partner)
            move((jp, rows), 2, partner)

        def three():
            landed(buf.at[0, rows], sem(1))
            move((j2, rows), 2, partner)

        def four():
            landed(buf.at[pl.ds(0, 4), rows], sem(2))

        def drain():
            landed(buf.at[pl.ds(0, 7), rows], sem(3))

        return one, two, three, four, drain

    top, bottom = pl.ds(0, H), pl.ds(H, H)

    def rs(k):
        sem = lambda n: rs_sem.at[k, n]
        both = lambda n: part_own[k, n].astype(F32) + from_core[k, n].astype(F32)

        def zero(term):
            for n in range(4):
                part_out[k, n] = term(n, other).astype(BF16)
            send(part_out.at[k], from_core.at[k], sem(3), sem(0), partner)
            for n in range(4):
                part_own[k, n] = term(n, core).astype(BF16)

        def one():
            landed(from_core.at[k], sem(0))
            half_sent[k] = both(y2).astype(BF16)
            send(half_sent.at[k, top], half_got.at[k, top], sem(4), sem(1), y_up)
            send(half_sent.at[k, bottom], half_got.at[k, bottom], sem(4), sem(1), y_down)

        def two():
            landed(half_got.at[k], sem(1))
            up, down = both(yp), both(ym)
            got = half_got[k].astype(F32)
            full_sent[k, 0] = jnp.concatenate([up[:H] + got[:H], up[H:]], axis=0).astype(BF16)
            send(full_sent.at[k, 0], full_got.at[k, 0], sem(5), sem(2), y_up)
            full_sent[k, 1] = jnp.concatenate([down[:H], down[H:] + got[H:]], axis=0).astype(BF16)
            send(full_sent.at[k, 1], full_got.at[k, 1], sem(5), sem(2), y_down)

        def three():
            landed(full_got.at[k], sem(2))
            return both(y) + (full_got[k, 0].astype(F32) + full_got[k, 1].astype(F32))

        def drain():
            landed(part_out.at[k], sem(3))
            landed(half_sent.at[k], sem(4))
            landed(full_sent.at[k], sem(5))

        return zero, one, two, three, drain

    def norm(buf, gain, first, count):
        step = 32

        def body(i, _):
            rows = pl.ds(pl.multiple_of(first + i * step, step), step)
            total = jnp.zeros((step, CH), F32)
            for j in range(8):
                v = buf[j, rows, :].astype(F32)
                total = total + v * v
            inverse = lax.rsqrt(jnp.sum(total, axis=-1, keepdims=True) * (1.0 / D) + NORM_EPSILON)
            for j in range(8):
                v = buf[j, rows, :].astype(F32)
                normed[rows, CH * j : CH * (j + 1)] = (v * inverse * gain[:, CH * j : CH * (j + 1)]).astype(BF16)
            return 0

        lax.fori_loop(0, count // step, body, 0)

    def project(m, _):
        rows = pl.ds(pl.multiple_of(m * 256, 256), 256)
        lhs = normed[rows, :]
        branch = jnp.dot(lhs, w_rec[...].reshape(D, CH), preferred_element_type=F32)
        padded[pl.ds(pl.multiple_of(m * 256 + 8, 8), 256), :] = branch.astype(BF16).astype(F32)
        gate = jnp.dot(lhs, w_gate[...].reshape(D, CH), preferred_element_type=F32)
        gate_act[rows, :] = jax.nn.gelu(gate.astype(BF16).astype(F32), approximate=True)
        return 0

    def gates(m, _):
        rows = pl.ds(pl.multiple_of(m * 128, 128), 128)
        window = padded[pl.ds(pl.multiple_of(m * 128, 128), 136), :]
        running = jnp.zeros((128, CH), F32)
        for k in range(4):
            running = running + window[5 + k : 133 + k] * conv_taps[k : k + 1, :].astype(F32)
        conv = running.astype(BF16)
        recur = jax.nn.sigmoid(jnp.dot(conv, recur_map[0], preferred_element_type=F32))
        enter = jax.nn.sigmoid(jnp.dot(conv, input_map[0], preferred_element_type=F32))
        p = -decay_param[...]
        softplus = jnp.maximum(p, 0.0) + jnp.log1p(jnp.exp(-jnp.abs(p)))
        log_decay = -GATE_SCALE * recur * softplus
        a = jnp.exp(log_decay)
        s = jnp.sqrt(minus_expm1(2.0 * log_decay)) * (enter * conv.astype(F32))
        for half in range(2):
            cols = slice(128 * half, 128 * (half + 1))
            decay[half, rows, :] = a[:, cols]
            drive[half, rows, :] = s[:, cols]
        return 0

    def scan():
        def body(k, carry):
            new = []
            for half in range(2):
                h, p = carry[half]
                at = pl.ds(k, SEGS, SEG)
                a = decay[half, at, :]
                h = a * h + drive[half, at, :]
                p = a * p
                drive[half, at, :] = h
                decay[half, at, :] = p
                new.append((h, p))
            return tuple(new)

        start = (jnp.zeros((SEGS, 128), F32), jnp.ones((SEGS, 128), F32))
        lax.fori_loop(0, SEG, body, (start, start), unroll=8)
        for half in range(2):
            cols = slice(128 * half, 128 * (half + 1))
            carry = jnp.zeros((1, 128), F32)
            for n in range(SEGS):
                rows = slice(SEG * n, SEG * (n + 1))
                state = drive[half, rows, :] + decay[half, rows, :] * carry
                carry = state[SEG - 1 : SEG]
                mixed[rows, cols] = (state * gate_act[rows, cols]).astype(BF16)

    def out_term(c):
        lhs = mixed[pl.ds(c * R, R), :]

        def term(n, side):
            rhs = jnp.concatenate([w_out[n, 2 * side], w_out[n, 2 * side + 1]], axis=1)
            return jnp.dot(lhs, rhs, preferred_element_type=F32)

        return term

    def lift(c):
        lhs = normed[pl.ds(c * R, R), :]
        for n in range(FF // 256):
            rhs = w_up[:, :, :, 256 * n : 256 * (n + 1)].reshape(D, 256)
            lifted = jnp.maximum(jnp.dot(lhs, rhs, preferred_element_type=F32), 0.0)
            squared[:, 256 * n : 256 * (n + 1)] = (lifted * lifted).astype(BF16)

    def down_term(n, side):
        rhs = jnp.concatenate([w_down[n, 2 * side], w_down[n, 2 * side + 1]], axis=1)
        return jnp.dot(squared[...], rhs, preferred_element_type=F32)

    t1, t2, t3, t4, t_drain = ag(0, tok_all, 0, TOK)
    w1("rec")
    w1("gate")
    t1()
    w2("rec")
    w2("gate")
    w1("out")
    t2()
    w3("rec")
    w3("gate")
    w2("out")
    w4("rec")
    w4("gate")
    t3()
    w3("out")
    w1("up")
    t4()
    norm(tok_all, mixer_gain, 0, TOK)
    w4("out")
    padded[pl.ds(0, 8), :] = jnp.zeros((8, CH), F32)
    w5("rec")
    w5("gate")
    w2("up")
    lax.fori_loop(0, TOK // 256, project, 0)
    w3("up")
    w1("down")
    lax.fori_loop(0, TOK // 128, gates, 0)
    scan()
    w5("out")
    w4("up")
    w2("down")

    mixer = [rs(c) for c in range(CHUNKS)]
    spread = [ag(1 + c, mid_all, c * R, R) for c in range(CHUNKS)]
    mlp = [rs(CHUNKS + c) for c in range(CHUNKS)]

    def middle(c):
        rows = pl.ds(c * R, R)
        total = mixer[c][3]()
        mid_all[tp, rows, :] = (tok_all[tp, rows, :].astype(F32) + total).astype(BF16)
        spread[c][0]()

    def feed(c):
        spread[c][3]()
        norm(mid_all, mlp_gain, c * R, R)
        if c == 0:
            w5("up")
        lift(c)
        if c == 0:
            w5("down")
        mlp[c][0](down_term)

    def finish(c):
        rows = pl.ds(c * R, R)
        result[rows, :] = (mid_all[tp, rows, :].astype(F32) + mlp[c][3]()).astype(BF16)

    stages = (
        lambda c: mixer[c][0](out_term(c)),
        lambda c: mixer[c][1](),
        lambda c: mixer[c][2](),
        middle,
        lambda c: spread[c][1](),
        lambda c: spread[c][2](),
        feed,
        lambda c: mlp[c][1](),
        lambda c: mlp[c][2](),
        finish,
    )
    for t in range(CHUNKS + len(stages) - 1):
        if t == 3:
            w3("down")
        if t == 5:
            w4("down")
        for n, stage in enumerate(stages):
            if 0 <= t - n < CHUNKS:
                stage(t - n)

    w_drain()
    t_drain()
    for group in (mixer, spread, mlp):
        for g in group:
            g[4]()


def shards(
    tokens,
    mixer_gain,
    rec_weight,
    gate_weight,
    conv_taps,
    recur_map,
    input_map,
    decay_param,
    out_weight,
    mlp_gain,
    up_weight,
    down_weight,
):
    hbm = pl.BlockSpec(memory_space=pl.ANY)
    vmem = pl.BlockSpec(memory_space=pltpu.VMEM)
    sums = 2 * CHUNKS
    return pl.pallas_call(
        kernel,
        out_shape=jax.ShapeDtypeStruct((TOK, CH), BF16),
        in_specs=[hbm] * 6 + [vmem] * 6,
        out_specs=vmem,
        scratch_shapes=[
            pltpu.VMEM((4, 4, D // 16, CH), BF16),
            pltpu.VMEM((4, 4, D // 16, CH), BF16),
            pltpu.VMEM((4, 4, CH, D // 16), BF16),
            pltpu.VMEM((4, 4, D // 16, FF), BF16),
            pltpu.VMEM((4, 4, FF, D // 16), BF16),
            pltpu.VMEM((8, TOK, CH), BF16),
            pltpu.VMEM((8, TOK, CH), BF16),
            pltpu.VMEM((TOK, D), BF16),
            pltpu.VMEM((TOK + 8, CH), F32),
            pltpu.VMEM((TOK, CH), F32),
            pltpu.VMEM((2, TOK, 128), F32),
            pltpu.VMEM((2, TOK, 128), F32),
            pltpu.VMEM((TOK, CH), BF16),
            pltpu.VMEM((R, FF), BF16),
            pltpu.VMEM((sums, 4, R, CH), BF16),
            pltpu.VMEM((sums, 4, R, CH), BF16),
            pltpu.VMEM((sums, 4, R, CH), BF16),
            pltpu.VMEM((sums, R, CH), BF16),
            pltpu.VMEM((sums, R, CH), BF16),
            pltpu.VMEM((sums, 2, R, CH), BF16),
            pltpu.VMEM((sums, 2, R, CH), BF16),
            pltpu.SemaphoreType.DMA((6,)),
            pltpu.SemaphoreType.DMA((5, 7)),
            pltpu.SemaphoreType.DMA((1 + CHUNKS, 4)),
            pltpu.SemaphoreType.DMA((sums, 6)),
        ],
        compiler_params=pltpu.CompilerParams(
            collective_id=0, has_side_effects=True, vmem_limit_bytes=60 * 1024 * 1024
        ),
    )(
        tokens,
        rec_weight,
        gate_weight,
        out_weight,
        up_weight,
        down_weight,
        mixer_gain.reshape(1, D),
        conv_taps,
        recur_map,
        input_map,
        decay_param.reshape(1, CH),
        mlp_gain.reshape(1, D),
    )


def solution(mesh):
    placed = (
        P(("rep", "fs"), "tp"),
        P(),
        P("fs", "tp"),
        P("fs", "tp"),
        P(None, "tp"),
        P("tp", None, None),
        P("tp", None, None),
        P("tp"),
        P("tp", "fs"),
        P(),
        P("fs", "tp"),
        P("tp", "fs"),
    )
    return jax.shard_map(
        shards, mesh=mesh, in_specs=placed, out_specs=P(("rep", "fs"), "tp"), check_vma=False
    )
```

```python
import jax
import jax.numpy as jnp
from jax import lax
from jax.experimental import pallas as pl
from jax.experimental.pallas import tpu as pltpu
from jax.sharding import PartitionSpec as P

NORM_EPSILON = 1e-06
GATE_SCALE = 8.0
MESH = pl.DeviceIdType.MESH
F32 = jnp.float32
BF16 = jnp.bfloat16

TOK = 768
D = 2048
CH = 256
FF = 1024
CHUNKS = 4
PARTS = 3
PART = TOK // PARTS
R = TOK // CHUNKS
H = R // 2
SEGS = 16
SEG = PART // SEGS


def send(src, dst, send_sem, recv_sem, device):
    pltpu.make_async_remote_copy(
        src_ref=src,
        dst_ref=dst,
        send_sem=send_sem,
        recv_sem=recv_sem,
        device_id=device,
        device_id_type=MESH,
    ).start()


def landed(ref, sem):
    with jax.named_scope("wait"):
        pltpu.make_async_copy(ref, ref, sem).wait()


def minus_expm1(u):
    series = 1.0 + u * (1.0 / 8.0)
    for k in (7.0, 6.0, 5.0, 4.0, 3.0, 2.0):
        series = 1.0 + (u * (1.0 / k)) * series
    return jnp.where(u > -0.5, -u * series, 1.0 - jnp.exp(u))


def kernel(
    tokens,
    rec_shard,
    gate_shard,
    out_shard,
    up_shard,
    down_shard,
    mixer_gain_in,
    conv_taps_in,
    recur_map_in,
    input_map_in,
    decay_param_in,
    mlp_gain_in,
    result,
    mixer_gain,
    conv_taps,
    recur_map,
    input_map,
    decay_param,
    mlp_gain,
    w_rec,
    w_gate,
    w_out,
    w_up,
    w_d0,
    w_d1,
    down_raw,
    w_dn,
    tok_all,
    mid_all,
    normed,
    padded,
    gate_act,
    decay,
    drive,
    mixed,
    squared,
    first_sum,
    m_part,
    m_core,
    m_half_sent,
    m_half_got,
    m_full_sent,
    m_full_got,
    f_part,
    f_core,
    f_half_sent,
    f_half_got,
    f_full_sent,
    f_full_got,
    local_sem,
    w_sem,
    w_sent,
    ag_sem,
    ag_sent,
    m_sem,
    m_sent,
    f_sem,
    f_sent,
):
    rep, fs, tp = lax.axis_index("rep"), lax.axis_index("fs"), lax.axis_index("tp")
    z, x = lax.div(fs, 4), lax.rem(fs, 4)
    y, core = lax.div(tp, 2), lax.rem(tp, 2)
    other = 1 - core
    xp, xm, x2 = lax.rem(x + 1, 4), lax.rem(x + 3, 4), lax.rem(x + 2, 4)
    zp, zm, z2 = lax.rem(z + 1, 4), lax.rem(z + 3, 4), lax.rem(z + 2, 4)
    yp, ym, y2 = lax.rem(y + 1, 4), lax.rem(y + 3, 4), lax.rem(y + 2, 4)
    deep = rep * 4 + z
    deep_p, deep_m = lax.rem(deep + 1, 8), lax.rem(deep + 7, 8)
    x_up, x_down = (rep, z * 4 + xp, tp), (rep, z * 4 + xm, tp)
    z_up = (lax.div(deep_p, 4), zp * 4 + x, tp)
    z_down = (lax.div(deep_m, 4), zm * 4 + x, tp)
    y_up, y_down = (rep, fs, yp * 2 + core), (rep, fs, ym * 2 + core)
    partner = (rep, fs, y * 2 + other)

    places = (
        (tokens, tok_all.at[tp]),
        (rec_shard, w_rec.at[z * 4 + x]),
        (gate_shard, w_gate.at[z * 4 + x]),
        (out_shard, w_out.at[z * 4 + x]),
        (up_shard, w_up.at[z * 4 + x]),
        (down_shard, down_raw),
        (mixer_gain_in, mixer_gain),
        (conv_taps_in, conv_taps),
        (recur_map_in, recur_map),
        (input_map_in, input_map),
        (decay_param_in, decay_param),
        (mlp_gain_in, mlp_gain),
    )
    fills = [pltpu.make_async_copy(s, d, local_sem.at[k]) for k, (s, d) in enumerate(places)]
    for fill in fills:
        fill.start()
    barrier = pltpu.get_barrier_semaphore()
    with jax.named_scope("barrier"):
        for device in (x_up, x_down, z_up, z_down, y_up, y_down, partner):
            pl.semaphore_signal(barrier, inc=1, device_id=device, device_id_type=MESH)
        pl.semaphore_wait(barrier, 7)
    for fill in fills:
        fill.wait()

    def copies(k, w, recv, *moves):
        for (i, j, rows), device in moves:
            ref = w.at[i * 4 + j, rows]
            send(ref, ref, w_sent.at[k], w_sem.at[k, recv], device)

    weights = {"rec": (0, w_rec), "gate": (1, w_gate), "out": (2, w_out), "up": (3, w_up), "d0": (4, w_d0), "d1": (5, w_d1)}

    def pieces(w):
        h = w.shape[1] // 2
        q = h // 2
        return pl.ds(0, h), pl.ds(h, h), pl.ds(0, q), pl.ds(q, q), pl.ds(h, q), pl.ds(h + q, q)

    def w1(name):
        k, w = weights[name]
        a, b, _, _, _, _ = pieces(w)
        copies(k, w, 0, ((z, x, a), x_up), ((z, x, a), x_down), ((z, x, b), z_up), ((z, x, b), z_down))
        copies(k, w, 2, ((z, x, a), z_up), ((z, x, a), z_down), ((z, x, b), x_up), ((z, x, b), x_down))

    def w2(name):
        k, w = weights[name]
        a, b, at, ab, bt, bb = pieces(w)
        landed(w.at[pl.ds(0, 2)], w_sem.at[k, 0])
        copies(k, w, 1, ((z, xm, at), x_up), ((z, xp, ab), x_down), ((zm, x, bt), z_up), ((zp, x, bb), z_down))
        for n in (xm, xp):
            copies(k, w, 2, ((z, n, a), z_up), ((z, n, a), z_down))
        for n in (zm, zp):
            copies(k, w, 2, ((n, x, b), x_up), ((n, x, b), x_down))

    def w3(name):
        k, w = weights[name]
        a, b, _, _, _, _ = pieces(w)
        landed(w.at[0], w_sem.at[k, 1])
        copies(k, w, 4, ((z, x2, a), z_up), ((z, x2, a), z_down), ((z2, x, b), x_up), ((z2, x, b), x_down))

    def w4(name):
        k, w = weights[name]
        _, _, at, ab, bt, bb = pieces(w)
        landed(w.at[pl.ds(0, 6)], w_sem.at[k, 2])
        for n in (x, xm, xp):
            copies(k, w, 3, ((zm, n, at), z_up), ((zp, n, ab), z_down))
        for n in (z, zm, zp):
            copies(k, w, 3, ((n, xm, bt), x_up), ((n, xp, bb), x_down))

    def w6(name):
        k, w = weights[name]
        _, _, at, ab, bt, bb = pieces(w)
        landed(w.at[pl.ds(0, 2)], w_sem.at[k, 4])
        copies(k, w, 3, ((zm, x2, at), z_up), ((zp, x2, ab), z_down), ((z2, xm, bt), x_up), ((z2, xp, bb), x_down))

    def w5(name):
        k, w = weights[name]
        landed(w.at[pl.ds(0, 4)], w_sem.at[k, 3])

    def w_drain():
        for k, w in weights.values():
            landed(w.at[pl.ds(0, 15)], w_sent.at[k])

    jp, jm, j2 = yp * 2 + core, ym * 2 + core, y2 * 2 + core

    def ag(k, buf, first, count, sent):
        rows, top, bottom = pl.ds(first, count), pl.ds(first, count // 2), pl.ds(first + count // 2, count // 2)
        sem = lambda n: ag_sem.at[k, n]
        move = lambda index, recv, device: send(buf.at[index], buf.at[index], sent, sem(recv), device)

        def one():
            move((tp, rows), 0, y_up)
            move((tp, rows), 0, y_down)
            move((tp, rows), 2, partner)

        def two():
            landed(buf.at[pl.ds(0, 2), rows], sem(0))
            move((jm, top), 1, y_up)
            move((jp, bottom), 1, y_down)
            move((jm, rows), 2, partner)
            move((jp, rows), 2, partner)

        def three():
            landed(buf.at[0, rows], sem(1))
            move((j2, rows), 2, partner)

        def four():
            landed(buf.at[pl.ds(0, 4), rows], sem(2))

        return one, two, three, four

    top, bottom = pl.ds(0, H), pl.ds(H, H)

    def rs(k, part, from_core, half_sent, half_got, full_sent, full_got, sems, sent):
        sem = lambda n: sems.at[k, n]
        both = lambda n: part[k, core, n].astype(F32) + from_core[k, n].astype(F32)

        def start():
            send(part.at[k, other], from_core.at[k], sent.at[0], sem(0), partner)

        def one():
            landed(from_core.at[k], sem(0))
            half_sent[k] = both(y2).astype(BF16)
            send(half_sent.at[k, top], half_got.at[k, top], sent.at[1], sem(1), y_up)
            send(half_sent.at[k, bottom], half_got.at[k, bottom], sent.at[1], sem(1), y_down)

        def two():
            landed(half_got.at[k], sem(1))
            up, down = both(yp), both(ym)
            got = half_got[k].astype(F32)
            full_sent[k, 0] = jnp.concatenate([up[:H] + got[:H], up[H:]], axis=0).astype(BF16)
            send(full_sent.at[k, 0], full_got.at[k, 0], sent.at[2], sem(2), y_up)
            full_sent[k, 1] = jnp.concatenate([down[:H], down[H:] + got[H:]], axis=0).astype(BF16)
            send(full_sent.at[k, 1], full_got.at[k, 1], sent.at[2], sem(2), y_down)

        def three():
            landed(full_got.at[k], sem(2))
            return both(y) + (full_got[k, 0].astype(F32) + full_got[k, 1].astype(F32))

        return start, one, two, three

    def norm(buf, gain, first, count):
        step = 64

        def body(i, _):
            rows = pl.ds(pl.multiple_of(first + i * step, step), step)
            total = jnp.zeros((step, CH), F32)
            for j in range(8):
                v = buf[j, rows, :].astype(F32)
                total = total + v * v
            inverse = lax.rsqrt(jnp.sum(total, axis=-1, keepdims=True) * (1.0 / D) + NORM_EPSILON)
            for j in range(8):
                v = buf[j, rows, :].astype(F32)
                normed[rows, CH * j : CH * (j + 1)] = (v * inverse * gain[:, CH * j : CH * (j + 1)]).astype(BF16)
            return 0

        lax.fori_loop(0, count // step, body, 0)

    def project(m):
        rows = pl.ds(m * 256, 256)
        lhs = normed[rows, :]
        branch = jnp.dot(lhs, w_rec[...].reshape(D, CH), preferred_element_type=F32)
        padded[pl.ds(m * 256 + 8, 256), :] = branch.astype(BF16).astype(F32)
        gate = jnp.dot(lhs, w_gate[...].reshape(D, CH), preferred_element_type=F32)
        gate_act[rows, :] = jax.nn.gelu(gate.astype(BF16).astype(F32), approximate=True)

    def gates(m, _):
        rows = pl.ds(pl.multiple_of(m * 128, 128), 128)
        window = padded[pl.ds(pl.multiple_of(m * 128, 128), 136), :]
        running = jnp.zeros((128, CH), F32)
        for k in range(4):
            running = running + window[5 + k : 133 + k] * conv_taps[k : k + 1, :].astype(F32)
        conv = running.astype(BF16)
        recur = jax.nn.sigmoid(jnp.dot(conv, recur_map[0], preferred_element_type=F32))
        enter = jax.nn.sigmoid(jnp.dot(conv, input_map[0], preferred_element_type=F32))
        p = -decay_param[...]
        softplus = jnp.maximum(p, 0.0) + jnp.log1p(jnp.exp(-jnp.abs(p)))
        log_decay = -GATE_SCALE * recur * softplus
        a = jnp.exp(log_decay)
        s = jnp.sqrt(minus_expm1(2.0 * log_decay)) * (enter * conv.astype(F32))
        for half in range(2):
            cols = slice(128 * half, 128 * (half + 1))
            decay[half, rows, :] = a[:, cols]
            drive[half, rows, :] = s[:, cols]
        return 0

    carries = [jnp.zeros((1, 128), F32)] * 2

    def scan(m):
        base = m * PART

        def body(k, carry):
            new = []
            for half in range(2):
                h, p = carry[half]
                at = pl.ds(base + k, SEGS, SEG)
                a = decay[half, at, :]
                h = a * h + drive[half, at, :]
                p = a * p
                drive[half, at, :] = h
                decay[half, at, :] = p
                new.append((h, p))
            return tuple(new)

        first = (jnp.zeros((SEGS, 128), F32), jnp.ones((SEGS, 128), F32))
        lax.fori_loop(0, SEG, body, (first, first), unroll=8)
        for half in range(2):
            cols = slice(128 * half, 128 * (half + 1))
            carry = carries[half]
            for n in range(SEGS):
                rows = slice(base + SEG * n, base + SEG * (n + 1))
                state = drive[half, rows, :] + decay[half, rows, :] * carry
                carry = state[SEG - 1 : SEG]
                mixed[rows, cols] = (state * gate_act[rows, cols]).astype(BF16)
            carries[half] = carry

    def out_product(c):
        lhs = mixed[pl.ds(c * R, R), :]
        for side in (other, core):
            for n in range(4):
                rhs = jnp.concatenate([w_out[4 * n + 2 * side], w_out[4 * n + 2 * side + 1]], axis=1)
                m_part[c, side, n] = jnp.dot(lhs, rhs, preferred_element_type=F32).astype(BF16)
            if side is other:
                mixer[c][0]()

    def lift(c):
        lhs = normed[pl.ds(c * R, R), :]
        for n in range(FF // 256):
            rhs = w_up[:, :, 256 * n : 256 * (n + 1)].reshape(D, 256)
            lifted = jnp.maximum(jnp.dot(lhs, rhs, preferred_element_type=F32), 0.0)
            squared[pl.ds(c * R, R), 256 * n : 256 * (n + 1)] = (lifted * lifted).astype(BF16)

    def low_lanes(shape):
        return lax.broadcasted_iota(jnp.int32, shape, 1) < 64

    def pack():
        step = 128

        def body(i, _):
            upper = down_raw[pl.ds(pl.multiple_of(i * step, step), step), :].astype(F32)
            lower = down_raw[pl.ds(pl.multiple_of(i * step + FF // 2, step), step), :].astype(F32)
            low = low_lanes((step, 128))
            rows = pl.ds(pl.multiple_of(i * step, step), step)
            w_d0[z * 4 + x, rows, :] = jnp.where(low, upper, pltpu.roll(lower, 64, 1)).astype(BF16)
            w_d1[z * 4 + x, rows, :] = jnp.where(low, pltpu.roll(upper, 64, 1), lower).astype(BF16)
            return 0

        lax.fori_loop(0, FF // 2 // step, body, 0)

    def unpack_rows(g, n, side, first):
        w, step = (w_d0, w_d1)[g], FF // 4
        low = low_lanes((128, 128))
        cols = pl.ds(pl.multiple_of(128 * side, 128), 128)
        for k in range(step // 128):
            left = w[4 * n + 2 * side, pl.ds(first + 128 * k, 128), :].astype(F32)
            right = w[4 * n + 2 * side + 1, pl.ds(first + 128 * k, 128), :].astype(F32)
            w_dn[g, n, pl.ds(first + 128 * k, 128), cols] = jnp.where(low, left, pltpu.roll(right, 64, 1)).astype(BF16)
            w_dn[g, n, pl.ds(first + FF // 2 + 128 * k, 128), cols] = jnp.where(low, pltpu.roll(left, 64, 1), right).astype(BF16)

    def unpack(g, late):
        pair = lax.div(x, 2)

        def body(i, _):
            if late:
                unpack_rows(g, i, 1 - pair, FF // 4)
            else:
                unpack_rows(g, i, pair, FF // 4)
            return 0

        lax.fori_loop(0, 4, body, 0)
        for n in (z2,) if late else (z, zm, zp):
            for side in range(2):
                unpack_rows(g, n, side, 0)

    def down_product(g, c):
        k = g * CHUNKS + c
        lhs = squared[pl.ds(c * R, R), :]
        for n in range(4):
            product = jnp.dot(lhs, w_dn[g, n], preferred_element_type=F32).astype(BF16)
            f_part[k, 0, n] = product[:, :128]
            f_part[k, 1, n] = product[:, 128:]
        mlp[k][0]()

    parts = [ag(n, tok_all, n * PART, PART, ag_sent.at[0]) for n in range(PARTS)]
    spread = [ag(PARTS + c, mid_all, c * R, R, ag_sent.at[1]) for c in range(CHUNKS)]
    m_bufs = (m_part, m_core, m_half_sent, m_half_got, m_full_sent, m_full_got, m_sem, m_sent)
    f_bufs = (f_part, f_core, f_half_sent, f_half_got, f_full_sent, f_full_got, f_sem, f_sent)
    mixer = [rs(c, *m_bufs) for c in range(CHUNKS)]
    mlp = [rs(k, *f_bufs) for k in range(2 * CHUNKS)]

    def middle(c):
        rows = pl.ds(c * R, R)
        total = mixer[c][3]()
        mid_all[tp, rows, :] = (tok_all[tp, rows, :].astype(F32) + total).astype(BF16)
        spread[c][0]()

    def feed(c):
        spread[c][3]()
        norm(mid_all, mlp_gain, c * R, R)
        lift(c)

    def finish(g, c):
        rows = pl.ds(c * R, R)
        total = mlp[g * CHUNKS + c][3]()
        if g == 0:
            first_sum[rows, :] = total
        else:
            early, low = first_sum[rows, :], low_lanes((R, 128))
            left = jnp.where(low, early, pltpu.roll(total, 64, 1))
            right = jnp.where(low, pltpu.roll(early, 64, 1), total)
            result[rows, :128] = (mid_all[tp, rows, :128].astype(F32) + left).astype(BF16)
            result[rows, 128:] = (mid_all[tp, rows, 128:].astype(F32) + right).astype(BF16)

    w_steps = {"w1": w1, "w2": w2, "w3": w3, "w4": w4, "w5": w5, "w6": w6}

    def part_start(m):
        norm(tok_all, mixer_gain, m * PART, PART)
        if m == 0:
            padded[pl.ds(0, 8), :] = jnp.zeros((8, CH), F32)
            w5("rec")
            w5("gate")
        project(m)

    def part_end(m):
        lax.fori_loop(2 * m, 2 * m + 2, gates, 0)
        scan(m)

    m_steps = (
        out_product,
        lambda c: mixer[c][1](),
        lambda c: mixer[c][2](),
        middle,
        lambda c: spread[c][1](),
        lambda c: spread[c][2](),
        feed,
    )

    def f_step(stage, g, c):
        if stage == 0:
            down_product(g, c)
        elif stage == 3:
            finish(g, c)
        else:
            mlp[g * CHUNKS + c][stage]()

    def do(*words):
        for word in words:
            with jax.named_scope(word):
                kind, digits = word[0], [int(d) for d in word[1:] if d.isdigit()]
                if kind == "w":
                    w_steps[word[:2]](word[3:])
                elif kind == "t":
                    parts[digits[1]][digits[0] - 1]()
                elif kind == "p":
                    pack()
                elif kind == "n":
                    part_start(*digits)
                elif kind == "g":
                    part_end(*digits)
                elif kind == "m":
                    m_steps[digits[0]](digits[1])
                elif kind == "u":
                    unpack(*digits)
                else:
                    f_step(*digits)

    do("w1_rec", "w1_gate", "t10", "t11", "t12", "w1_out", "p", "w2_rec", "w2_gate", "t20", "w2_out", "w3_rec", "w3_gate", "t21")
    do("w4_rec", "w4_gate", "w3_out", "t22", "w6_rec", "w6_gate", "t30", "w4_out", "w6_out", "w1_up", "w1_d0", "t31", "t40", "n0")
    do("t32", "g0", "w5_out", "m00", "t41", "n1", "w2_up", "m10", "g1", "m01", "t42", "n2", "m20", "m11", "g2", "m02", "m03")
    do("m12", "m13", "m30", "w3_up", "w2_d0", "m21", "m22", "w4_up", "m31", "w6_up", "w1_d1", "m40", "m23", "m32", "w3_d0", "w4_d0")
    do("m50", "m41", "m33", "w5_up", "m60", "w2_d1", "m51", "m42", "w6_d0", "m61", "m43", "u00", "m52", "w3_d1", "m62", "m53")
    do("w4_d1", "w5_d0", "u01", "f000", "f001", "f100", "w6_d1", "m63", "f002", "f101", "f003", "f102", "f103", "u10", "f200", "f201")
    do("w5_d1", "u11", "f202", "f203", "f010", "f011", "f110", "f012", "f111", "f013", "f112", "f113", "f300", "f301", "f302", "f303")
    do("f210", "f211", "f212", "f213", "f310", "f311", "f312", "f313")

    with jax.named_scope("drain"):
        w_drain()
        landed(tok_all.at[pl.ds(0, 7)], ag_sent.at[0])
        landed(mid_all.at[pl.ds(0, 7)], ag_sent.at[1])
        for bufs in (m_bufs, f_bufs):
            _, from_core, half_sent, _, full_sent, _, _, sent = bufs
            landed(from_core, sent.at[0])
            landed(half_sent, sent.at[1])
            landed(full_sent, sent.at[2])


def shards(
    tokens,
    mixer_gain,
    rec_weight,
    gate_weight,
    conv_taps,
    recur_map,
    input_map,
    decay_param,
    out_weight,
    mlp_gain,
    up_weight,
    down_weight,
):
    hbm = pl.BlockSpec(memory_space=pl.ANY)

    def sums(count, width):
        shapes = [(2, 4, R, width), (4, R, width), (R, width), (R, width), (2, R, width), (2, R, width)]
        return [pltpu.VMEM((count, *shape), BF16) for shape in shapes]

    return pl.pallas_call(
        kernel,
        out_shape=pltpu.VMEM((TOK, CH), BF16),
        in_specs=[hbm] * 12,
        out_specs=pl.BlockSpec(memory_space=pltpu.VMEM),
        scratch_shapes=[
            pltpu.VMEM((1, D), F32),
            pltpu.VMEM((4, CH), BF16),
            pltpu.VMEM((1, CH, CH), BF16),
            pltpu.VMEM((1, CH, CH), BF16),
            pltpu.VMEM((1, CH), F32),
            pltpu.VMEM((1, D), F32),
            pltpu.VMEM((16, D // 16, CH), BF16),
            pltpu.VMEM((16, D // 16, CH), BF16),
            pltpu.VMEM((16, CH, D // 16), BF16),
            pltpu.VMEM((16, D // 16, FF), BF16),
            pltpu.VMEM((16, FF // 2, D // 16), BF16),
            pltpu.VMEM((16, FF // 2, D // 16), BF16),
            pltpu.VMEM((FF, D // 16), BF16),
            pltpu.VMEM((2, 4, FF, CH), BF16),
            pltpu.VMEM((8, TOK, CH), BF16),
            pltpu.VMEM((8, TOK, CH), BF16),
            pltpu.VMEM((TOK, D), BF16),
            pltpu.VMEM((TOK + 8, CH), F32),
            pltpu.VMEM((TOK, CH), F32),
            pltpu.VMEM((2, TOK, 128), F32),
            pltpu.VMEM((2, TOK, 128), F32),
            pltpu.VMEM((TOK, CH), BF16),
            pltpu.VMEM((TOK, FF), BF16),
            pltpu.VMEM((TOK, 128), F32),
            *sums(CHUNKS, CH),
            *sums(2 * CHUNKS, CH // 2),
            pltpu.SemaphoreType.DMA((12,)),
            pltpu.SemaphoreType.DMA((6, 5)),
            pltpu.SemaphoreType.DMA((6,)),
            pltpu.SemaphoreType.DMA((PARTS + CHUNKS, 3)),
            pltpu.SemaphoreType.DMA((2,)),
            pltpu.SemaphoreType.DMA((CHUNKS, 3)),
            pltpu.SemaphoreType.DMA((3,)),
            pltpu.SemaphoreType.DMA((2 * CHUNKS, 3)),
            pltpu.SemaphoreType.DMA((3,)),
        ],
        compiler_params=pltpu.CompilerParams(
            collective_id=0, has_side_effects=True, vmem_limit_bytes=60 * 1024 * 1024
        ),
    )(
        tokens,
        rec_weight,
        gate_weight,
        out_weight,
        up_weight,
        down_weight,
        mixer_gain.reshape(1, D),
        conv_taps,
        recur_map,
        input_map,
        decay_param.reshape(1, CH),
        mlp_gain.reshape(1, D),
    )


def solution(mesh):
    placed = (
        P(("rep", "fs"), "tp"),
        P(),
        P("fs", "tp"),
        P("fs", "tp"),
        P(None, "tp"),
        P("tp", None, None),
        P("tp", None, None),
        P("tp"),
        P("tp", "fs"),
        P(),
        P("fs", "tp"),
        P("tp", "fs"),
    )
    return jax.shard_map(
        shards, mesh=mesh, in_specs=placed, out_specs=P(("rep", "fs"), "tp"), check_vma=False
    )
```

```python
import jax
import jax.numpy as jnp
from jax import lax
from jax.experimental import pallas as pl
from jax.experimental.pallas import tpu as pltpu
from jax.sharding import PartitionSpec as P

NORM_EPSILON = 1e-06
GATE_SCALE = 8.0
MESH = pl.DeviceIdType.MESH
F32 = jnp.float32
BF16 = jnp.bfloat16

TOK = 768
D = 2048
CH = 256
FF = 1024
CHUNKS = 4
PARTS = 3
PART = TOK // PARTS
R = TOK // CHUNKS
H = R // 2
SEGS = 16
SEG = PART // SEGS


def send(src, dst, send_sem, recv_sem, device):
    pltpu.make_async_remote_copy(
        src_ref=src,
        dst_ref=dst,
        send_sem=send_sem,
        recv_sem=recv_sem,
        device_id=device,
        device_id_type=MESH,
    ).start()


def landed(ref, sem):
    with jax.named_scope("wait"):
        pltpu.make_async_copy(ref, ref, sem).wait()


def minus_expm1(u):
    series = 1.0 + u * (1.0 / 8.0)
    for k in (7.0, 6.0, 5.0, 4.0, 3.0, 2.0):
        series = 1.0 + (u * (1.0 / k)) * series
    return jnp.where(u > -0.5, -u * series, 1.0 - jnp.exp(u))


def kernel(
    tokens,
    rec_shard,
    gate_shard,
    out_shard,
    up_shard,
    down_shard,
    mixer_gain_in,
    conv_taps_in,
    recur_map_in,
    input_map_in,
    decay_param_in,
    mlp_gain_in,
    result,
    mixer_gain,
    conv_taps,
    recur_map,
    input_map,
    decay_param,
    mlp_gain,
    w_rec,
    w_gate,
    w_out,
    w_up,
    w_d0,
    w_d1,
    down_raw,
    w_dn,
    tok_all,
    mid_all,
    normed,
    padded,
    gate_act,
    decay,
    drive,
    mixed,
    squared,
    first_sum,
    m_part,
    m_core,
    m_half_sent,
    m_half_got,
    m_full_sent,
    m_full_got,
    f_part,
    f_core,
    f_half_sent,
    f_half_got,
    f_full_sent,
    f_full_got,
    local_sem,
    w_sem,
    w_sent,
    ag_sem,
    ag_sent,
    m_sem,
    m_sent,
    f_sem,
    f_sent,
):
    rep, fs, tp = lax.axis_index("rep"), lax.axis_index("fs"), lax.axis_index("tp")
    z, x = lax.div(fs, 4), lax.rem(fs, 4)
    y, core = lax.div(tp, 2), lax.rem(tp, 2)
    other = 1 - core
    xp, xm, x2 = lax.rem(x + 1, 4), lax.rem(x + 3, 4), lax.rem(x + 2, 4)
    zp, zm, z2 = lax.rem(z + 1, 4), lax.rem(z + 3, 4), lax.rem(z + 2, 4)
    yp, ym, y2 = lax.rem(y + 1, 4), lax.rem(y + 3, 4), lax.rem(y + 2, 4)
    deep = rep * 4 + z
    deep_p, deep_m = lax.rem(deep + 1, 8), lax.rem(deep + 7, 8)
    x_up, x_down = (rep, z * 4 + xp, tp), (rep, z * 4 + xm, tp)
    z_up = (lax.div(deep_p, 4), zp * 4 + x, tp)
    z_down = (lax.div(deep_m, 4), zm * 4 + x, tp)
    y_up, y_down = (rep, fs, yp * 2 + core), (rep, fs, ym * 2 + core)
    partner = (rep, fs, y * 2 + other)

    places = (
        (tokens, tok_all.at[tp]),
        (rec_shard, w_rec.at[z * 4 + x]),
        (gate_shard, w_gate.at[z * 4 + x]),
        (out_shard, w_out.at[z * 4 + x]),
        (up_shard, w_up.at[z * 4 + x]),
        (down_shard, down_raw),
        (mixer_gain_in, mixer_gain),
        (conv_taps_in, conv_taps),
        (recur_map_in, recur_map),
        (input_map_in, input_map),
        (decay_param_in, decay_param),
        (mlp_gain_in, mlp_gain),
    )
    fills = [pltpu.make_async_copy(s, d, local_sem.at[k]) for k, (s, d) in enumerate(places)]
    for fill in fills:
        fill.start()
    barrier = pltpu.get_barrier_semaphore()
    with jax.named_scope("barrier"):
        for device in (x_up, x_down, z_up, z_down, y_up, y_down, partner):
            pl.semaphore_signal(barrier, inc=1, device_id=device, device_id_type=MESH)
        pl.semaphore_wait(barrier, 7)
    for fill in fills:
        fill.wait()

    def copies(k, w, recv, *moves):
        for (i, j, rows), device in moves:
            ref = w.at[i * 4 + j, rows]
            send(ref, ref, w_sent.at[k], w_sem.at[k, recv], device)

    weights = {"rec": (0, w_rec), "gate": (1, w_gate), "out": (2, w_out), "up": (3, w_up), "d0": (4, w_d0), "d1": (5, w_d1)}

    def pieces(w):
        h = w.shape[1] // 2
        q = h // 2
        return pl.ds(0, h), pl.ds(h, h), pl.ds(0, q), pl.ds(q, q), pl.ds(h, q), pl.ds(h + q, q)

    def w1(name):
        k, w = weights[name]
        a, b, _, _, _, _ = pieces(w)
        copies(k, w, 0, ((z, x, a), x_up), ((z, x, a), x_down), ((z, x, b), z_up), ((z, x, b), z_down))
        copies(k, w, 2, ((z, x, a), z_up), ((z, x, a), z_down), ((z, x, b), x_up), ((z, x, b), x_down))

    def w2(name):
        k, w = weights[name]
        a, b, at, ab, bt, bb = pieces(w)
        landed(w.at[pl.ds(0, 2)], w_sem.at[k, 0])
        copies(k, w, 1, ((z, xm, at), x_up), ((z, xp, ab), x_down), ((zm, x, bt), z_up), ((zp, x, bb), z_down))
        for n in (xm, xp):
            copies(k, w, 2, ((z, n, a), z_up), ((z, n, a), z_down))
        for n in (zm, zp):
            copies(k, w, 2, ((n, x, b), x_up), ((n, x, b), x_down))

    def w3(name):
        k, w = weights[name]
        a, b, _, _, _, _ = pieces(w)
        landed(w.at[0], w_sem.at[k, 1])
        copies(k, w, 4, ((z, x2, a), z_up), ((z, x2, a), z_down), ((z2, x, b), x_up), ((z2, x, b), x_down))

    def w4(name):
        k, w = weights[name]
        _, _, at, ab, bt, bb = pieces(w)
        landed(w.at[pl.ds(0, 6)], w_sem.at[k, 2])
        for n in (x, xm, xp):
            copies(k, w, 3, ((zm, n, at), z_up), ((zp, n, ab), z_down))
        for n in (z, zm, zp):
            copies(k, w, 3, ((n, xm, bt), x_up), ((n, xp, bb), x_down))

    def w6(name):
        k, w = weights[name]
        _, _, at, ab, bt, bb = pieces(w)
        landed(w.at[pl.ds(0, 2)], w_sem.at[k, 4])
        copies(k, w, 3, ((zm, x2, at), z_up), ((zp, x2, ab), z_down), ((z2, xm, bt), x_up), ((z2, xp, bb), x_down))

    def w5(name):
        k, w = weights[name]
        landed(w.at[pl.ds(0, 4)], w_sem.at[k, 3])

    def w_drain():
        for k, w in weights.values():
            landed(w.at[pl.ds(0, 15)], w_sent.at[k])

    jp, jm, j2 = yp * 2 + core, ym * 2 + core, y2 * 2 + core

    def ag(k, buf, first, count, sent):
        rows, top, bottom = pl.ds(first, count), pl.ds(first, count // 2), pl.ds(first + count // 2, count // 2)
        sem = lambda n: ag_sem.at[k, n]
        move = lambda index, recv, device: send(buf.at[index], buf.at[index], sent, sem(recv), device)

        def one():
            move((tp, rows), 0, y_up)
            move((tp, rows), 0, y_down)
            move((tp, rows), 2, partner)

        def two():
            landed(buf.at[pl.ds(0, 2), rows], sem(0))
            move((jm, top), 1, y_up)
            move((jp, bottom), 1, y_down)
            move((jm, rows), 2, partner)
            move((jp, rows), 2, partner)

        def three():
            landed(buf.at[0, rows], sem(1))
            move((j2, rows), 2, partner)

        def four():
            landed(buf.at[pl.ds(0, 4), rows], sem(2))

        return one, two, three, four

    top, bottom = pl.ds(0, H), pl.ds(H, H)

    def rs(k, part, from_core, half_sent, half_got, full_sent, full_got, sems, sent):
        sem = lambda n: sems.at[k, n]
        both = lambda n: part[k, core, n].astype(F32) + from_core[k, n].astype(F32)

        def start():
            send(part.at[k, other], from_core.at[k], sent.at[0], sem(0), partner)

        def one():
            landed(from_core.at[k], sem(0))
            half_sent[k] = both(y2).astype(BF16)
            send(half_sent.at[k, top], half_got.at[k, top], sent.at[1], sem(1), y_up)
            send(half_sent.at[k, bottom], half_got.at[k, bottom], sent.at[1], sem(1), y_down)

        def two():
            landed(half_got.at[k], sem(1))
            up, down = both(yp), both(ym)
            got = half_got[k].astype(F32)
            full_sent[k, 0] = jnp.concatenate([up[:H] + got[:H], up[H:]], axis=0).astype(BF16)
            send(full_sent.at[k, 0], full_got.at[k, 0], sent.at[2], sem(2), y_up)
            full_sent[k, 1] = jnp.concatenate([down[:H], down[H:] + got[H:]], axis=0).astype(BF16)
            send(full_sent.at[k, 1], full_got.at[k, 1], sent.at[2], sem(2), y_down)

        def three():
            landed(full_got.at[k], sem(2))
            return both(y) + (full_got[k, 0].astype(F32) + full_got[k, 1].astype(F32))

        return start, one, two, three

    def norm(buf, gain, first, count):
        step = count // 2

        def body(i, _):
            rows = pl.ds(pl.multiple_of(first + i * step, 32), step)
            total = jnp.zeros((step, CH), F32)
            for j in range(8):
                v = buf[j, rows, :].astype(F32)
                total = total + v * v
            inverse = lax.rsqrt(jnp.sum(total, axis=-1, keepdims=True) * (1.0 / D) + NORM_EPSILON)
            for j in range(8):
                v = buf[j, rows, :].astype(F32)
                normed[rows, CH * j : CH * (j + 1)] = (v * inverse * gain[:, CH * j : CH * (j + 1)]).astype(BF16)
            return 0

        lax.fori_loop(0, count // step, body, 0)

    def project(m):
        rows = pl.ds(m * 256, 256)
        lhs = normed[rows, :]
        branch = jnp.dot(lhs, w_rec[...].reshape(D, CH), preferred_element_type=F32)
        padded[pl.ds(m * 256 + 8, 256), :] = branch.astype(BF16).astype(F32)
        gate = jnp.dot(lhs, w_gate[...].reshape(D, CH), preferred_element_type=F32)
        gate_act[rows, :] = jax.nn.gelu(gate.astype(BF16).astype(F32), approximate=True)

    def gates(m, _):
        rows = pl.ds(pl.multiple_of(m * 128, 128), 128)
        window = padded[pl.ds(pl.multiple_of(m * 128, 128), 136), :]
        running = jnp.zeros((128, CH), F32)
        for k in range(4):
            running = running + window[5 + k : 133 + k] * conv_taps[k : k + 1, :].astype(F32)
        conv = running.astype(BF16)
        recur = jax.nn.sigmoid(jnp.dot(conv, recur_map[0], preferred_element_type=F32))
        enter = jax.nn.sigmoid(jnp.dot(conv, input_map[0], preferred_element_type=F32))
        p = -decay_param[...]
        softplus = jnp.maximum(p, 0.0) + jnp.log1p(jnp.exp(-jnp.abs(p)))
        log_decay = -GATE_SCALE * recur * softplus
        a = jnp.exp(log_decay)
        s = jnp.sqrt(minus_expm1(2.0 * log_decay)) * (enter * conv.astype(F32))
        for half in range(2):
            cols = slice(128 * half, 128 * (half + 1))
            decay[half, rows, :] = a[:, cols]
            drive[half, rows, :] = s[:, cols]
        return 0

    carries = [jnp.zeros((1, 128), F32)] * 2

    def scan(m):
        base = m * PART

        def body(k, carry):
            new = []
            for half in range(2):
                h, p = carry[half]
                at = pl.ds(base + k, SEGS, SEG)
                a = decay[half, at, :]
                h = a * h + drive[half, at, :]
                p = a * p
                drive[half, at, :] = h
                decay[half, at, :] = p
                new.append((h, p))
            return tuple(new)

        first = (jnp.zeros((SEGS, 128), F32), jnp.ones((SEGS, 128), F32))
        lax.fori_loop(0, SEG, body, (first, first), unroll=8)
        for half in range(2):
            cols = slice(128 * half, 128 * (half + 1))
            carry = carries[half]
            for n in range(SEGS):
                rows = slice(base + SEG * n, base + SEG * (n + 1))
                state = drive[half, rows, :] + decay[half, rows, :] * carry
                carry = state[SEG - 1 : SEG]
                mixed[rows, cols] = (state * gate_act[rows, cols]).astype(BF16)
            carries[half] = carry

    def out_product(c):
        lhs = mixed[pl.ds(c * R, R), :]
        for side in (other, core):
            for n in range(4):
                rhs = jnp.concatenate([w_out[4 * n + 2 * side], w_out[4 * n + 2 * side + 1]], axis=1)
                m_part[c, side, n] = jnp.dot(lhs, rhs, preferred_element_type=F32).astype(BF16)
            if side is other:
                mixer[c][0]()

    def lift(c):
        lhs = normed[pl.ds(c * R, R), :]
        for n in range(FF // 256):
            rhs = w_up[:, :, 256 * n : 256 * (n + 1)].reshape(D, 256)
            lifted = jnp.maximum(jnp.dot(lhs, rhs, preferred_element_type=F32), 0.0)
            squared[pl.ds(c * R, R), 256 * n : 256 * (n + 1)] = (lifted * lifted).astype(BF16)

    def low_lanes(shape):
        return lax.broadcasted_iota(jnp.int32, shape, 1) < 64

    def pack():
        step, odd = 128, lax.rem(x, 2)

        def body(i, _):
            upper = down_raw[pl.ds(pl.multiple_of(i * step + odd * (FF // 2), step), step), :].astype(F32)
            lower = down_raw[pl.ds(pl.multiple_of(i * step + (1 - odd) * (FF // 2), step), step), :].astype(F32)
            low = low_lanes((step, 128))
            rows = pl.ds(pl.multiple_of(i * step, step), step)
            w_d0[z * 4 + x, rows, :] = jnp.where(low, upper, pltpu.roll(lower, 64, 1)).astype(BF16)
            w_d1[z * 4 + x, rows, :] = jnp.where(low, pltpu.roll(upper, 64, 1), lower).astype(BF16)
            return 0

        lax.fori_loop(0, FF // 2 // step, body, 0)

    def unpack_rows(g, n, side, first):
        w, step = (w_d0, w_d1)[g], FF // 4
        low = low_lanes((128, 128))
        cols = pl.ds(pl.multiple_of(128 * side, 128), 128)
        for k in range(step // 128):
            left = w[4 * n + 2 * side, pl.ds(first + 128 * k, 128), :]
            right = w[4 * n + 2 * side + 1, pl.ds(first + 128 * k, 128), :]
            w_dn[g, n, pl.ds(first + 128 * k, 128), cols] = jnp.where(low, left, right)
            swapped = jnp.where(low, right, left).astype(F32)
            w_dn[g, n, pl.ds(first + FF // 2 + 128 * k, 128), cols] = pltpu.roll(swapped, 64, 1).astype(BF16)

    def unpack(g, late):
        pair = lax.div(x, 2)

        def body(i, _):
            if late:
                unpack_rows(g, i, 1 - pair, FF // 4)
            else:
                unpack_rows(g, i, pair, FF // 4)
            return 0

        lax.fori_loop(0, 4, body, 0)
        for n in (z2,) if late else (z, zm, zp):
            for side in range(2):
                unpack_rows(g, n, side, 0)

    def down_product(g, c):
        k = g * CHUNKS + c
        lhs = squared[pl.ds(c * R, R), :]
        for n in range(4):
            product = jnp.dot(lhs, w_dn[g, n], preferred_element_type=F32).astype(BF16)
            f_part[k, 0, n] = product[:, :128]
            f_part[k, 1, n] = product[:, 128:]
        mlp[k][0]()

    parts = [ag(n, tok_all, n * PART, PART, ag_sent.at[0]) for n in range(PARTS)]
    spread = [ag(PARTS + c, mid_all, c * R, R, ag_sent.at[1]) for c in range(CHUNKS)]
    m_bufs = (m_part, m_core, m_half_sent, m_half_got, m_full_sent, m_full_got, m_sem, m_sent)
    f_bufs = (f_part, f_core, f_half_sent, f_half_got, f_full_sent, f_full_got, f_sem, f_sent)
    mixer = [rs(c, *m_bufs) for c in range(CHUNKS)]
    mlp = [rs(k, *f_bufs) for k in range(2 * CHUNKS)]

    def middle(c):
        rows = pl.ds(c * R, R)
        total = mixer[c][3]()
        mid_all[tp, rows, :] = (tok_all[tp, rows, :].astype(F32) + total).astype(BF16)
        spread[c][0]()

    def feed(c):
        spread[c][3]()
        norm(mid_all, mlp_gain, c * R, R)
        lift(c)

    def finish(g, c):
        rows = pl.ds(c * R, R)
        total = mlp[g * CHUNKS + c][3]()
        if g == 0:
            first_sum[rows, :] = total
        else:
            early, low = first_sum[rows, :], low_lanes((R, 128))
            left = jnp.where(low, early, pltpu.roll(total, 64, 1))
            right = jnp.where(low, pltpu.roll(early, 64, 1), total)
            result[rows, :128] = (mid_all[tp, rows, :128].astype(F32) + left).astype(BF16)
            result[rows, 128:] = (mid_all[tp, rows, 128:].astype(F32) + right).astype(BF16)

    w_steps = {"w1": w1, "w2": w2, "w3": w3, "w4": w4, "w5": w5, "w6": w6}

    def part_start(m):
        if m == 0:
            padded[pl.ds(0, 8), :] = jnp.zeros((8, CH), F32)
            w5("rec")
            w5("gate")
        project(m)

    def part_end(m):
        lax.fori_loop(2 * m, 2 * m + 2, gates, 0)
        scan(m)

    m_steps = (
        out_product,
        lambda c: mixer[c][1](),
        lambda c: mixer[c][2](),
        middle,
        lambda c: spread[c][1](),
        lambda c: spread[c][2](),
        feed,
    )

    def f_step(stage, g, c):
        if stage == 0:
            down_product(g, c)
        elif stage == 3:
            finish(g, c)
        else:
            mlp[g * CHUNKS + c][stage]()

    def do(*words):
        for word in words:
            with jax.named_scope(word):
                kind, digits = word[0], [int(d) for d in word[1:] if d.isdigit()]
                if kind == "w":
                    w_steps[word[:2]](word[3:])
                elif kind == "t":
                    parts[digits[1]][digits[0] - 1]()
                elif kind == "p":
                    pack()
                elif kind == "a":
                    norm(tok_all, mixer_gain, digits[0] * PART, PART)
                elif kind == "n":
                    part_start(*digits)
                elif kind == "g":
                    part_end(*digits)
                elif kind == "m":
                    m_steps[digits[0]](digits[1])
                elif kind == "u":
                    unpack(*digits)
                else:
                    f_step(*digits)

    do("w1_rec", "w1_gate", "t10", "t11", "t12", "w1_out", "p", "w2_rec", "w2_gate", "t20", "w2_out", "w3_rec", "w3_gate", "t21")
    do("w4_rec", "w4_gate", "w3_out", "t22", "w6_rec", "w6_gate", "t30", "w4_out", "t31", "t40", "a0", "w6_out", "w1_up", "w1_d0")
    do("t41", "a1", "n0", "t32", "g0", "w5_out", "m00", "n1", "w2_up", "m10", "g1", "m01", "t42", "a2", "n2", "m20", "m11", "g2")
    do("m02", "m03", "m12", "m13", "m30", "w3_up", "w2_d0", "m21", "m22", "w4_up", "m31", "w6_up", "w3_d0", "w1_d1", "m40", "m23")
    do("w4_d0", "m32", "m50", "m41", "m33", "w5_up", "m60", "w6_d0", "w2_d1", "m51", "m42", "m61", "m43", "u00", "w3_d1", "m52")
    do("w5_d0", "u01", "f000", "f001", "f100", "w4_d1", "m53", "m62", "w6_d1", "f101", "f002", "m63", "f102", "f003", "f200", "f201")
    do("u10", "f103", "w5_d1", "u11", "f010", "f011", "f202", "f110", "f012", "f203", "f111", "f013", "f112", "f113", "f300", "f301")
    do("f210", "f302", "f211", "f303", "f212", "f213", "f310", "f311", "f312", "f313")

    with jax.named_scope("drain"):
        w_drain()
        landed(tok_all.at[pl.ds(0, 7)], ag_sent.at[0])
        landed(mid_all.at[pl.ds(0, 7)], ag_sent.at[1])
        for bufs in (m_bufs, f_bufs):
            _, from_core, half_sent, _, full_sent, _, _, sent = bufs
            landed(from_core, sent.at[0])
            landed(half_sent, sent.at[1])
            landed(full_sent, sent.at[2])


def shards(
    tokens,
    mixer_gain,
    rec_weight,
    gate_weight,
    conv_taps,
    recur_map,
    input_map,
    decay_param,
    out_weight,
    mlp_gain,
    up_weight,
    down_weight,
):
    hbm = pl.BlockSpec(memory_space=pl.ANY)

    def sums(count, width):
        shapes = [(2, 4, R, width), (4, R, width), (R, width), (R, width), (2, R, width), (2, R, width)]
        return [pltpu.VMEM((count, *shape), BF16) for shape in shapes]

    return pl.pallas_call(
        kernel,
        out_shape=pltpu.VMEM((TOK, CH), BF16),
        in_specs=[hbm] * 12,
        out_specs=pl.BlockSpec(memory_space=pltpu.VMEM),
        scratch_shapes=[
            pltpu.VMEM((1, D), F32),
            pltpu.VMEM((4, CH), BF16),
            pltpu.VMEM((1, CH, CH), BF16),
            pltpu.VMEM((1, CH, CH), BF16),
            pltpu.VMEM((1, CH), F32),
            pltpu.VMEM((1, D), F32),
            pltpu.VMEM((16, D // 16, CH), BF16),
            pltpu.VMEM((16, D // 16, CH), BF16),
            pltpu.VMEM((16, CH, D // 16), BF16),
            pltpu.VMEM((16, D // 16, FF), BF16),
            pltpu.VMEM((16, FF // 2, D // 16), BF16),
            pltpu.VMEM((16, FF // 2, D // 16), BF16),
            pltpu.VMEM((FF, D // 16), BF16),
            pltpu.VMEM((2, 4, FF, CH), BF16),
            pltpu.VMEM((8, TOK, CH), BF16),
            pltpu.VMEM((8, TOK, CH), BF16),
            pltpu.VMEM((TOK, D), BF16),
            pltpu.VMEM((TOK + 8, CH), F32),
            pltpu.VMEM((TOK, CH), F32),
            pltpu.VMEM((2, TOK, 128), F32),
            pltpu.VMEM((2, TOK, 128), F32),
            pltpu.VMEM((TOK, CH), BF16),
            pltpu.VMEM((TOK, FF), BF16),
            pltpu.VMEM((TOK, 128), F32),
            *sums(CHUNKS, CH),
            *sums(2 * CHUNKS, CH // 2),
            pltpu.SemaphoreType.DMA((12,)),
            pltpu.SemaphoreType.DMA((6, 5)),
            pltpu.SemaphoreType.DMA((6,)),
            pltpu.SemaphoreType.DMA((PARTS + CHUNKS, 3)),
            pltpu.SemaphoreType.DMA((2,)),
            pltpu.SemaphoreType.DMA((CHUNKS, 3)),
            pltpu.SemaphoreType.DMA((3,)),
            pltpu.SemaphoreType.DMA((2 * CHUNKS, 3)),
            pltpu.SemaphoreType.DMA((3,)),
        ],
        compiler_params=pltpu.CompilerParams(
            collective_id=0, has_side_effects=True, vmem_limit_bytes=60 * 1024 * 1024
        ),
    )(
        tokens,
        rec_weight,
        gate_weight,
        out_weight,
        up_weight,
        down_weight,
        mixer_gain.reshape(1, D),
        conv_taps,
        recur_map,
        input_map,
        decay_param.reshape(1, CH),
        mlp_gain.reshape(1, D),
    )


def solution(mesh):
    placed = (
        P(("rep", "fs"), "tp"),
        P(),
        P("fs", "tp"),
        P("fs", "tp"),
        P(None, "tp"),
        P("tp", None, None),
        P("tp", None, None),
        P("tp"),
        P("tp", "fs"),
        P(),
        P("fs", "tp"),
        P("tp", "fs"),
    )
    return jax.shard_map(
        shards, mesh=mesh, in_specs=placed, out_specs=P(("rep", "fs"), "tp"), check_vma=False
    )
```

```python
import jax
import jax.numpy as jnp
from jax import lax
from jax.experimental import pallas as pl
from jax.experimental.pallas import tpu as pltpu
from jax.sharding import PartitionSpec as P

NORM_EPSILON = 1e-06
GATE_SCALE = 8.0
MESH = pl.DeviceIdType.MESH
F32 = jnp.float32
BF16 = jnp.bfloat16

TOK = 768
D = 2048
CH = 256
FF = 1024
CHUNKS = 4
PARTS = 3
PART = TOK // PARTS
R = TOK // CHUNKS
H = R // 2
SEGS = 16
SEG = PART // SEGS


def send(src, dst, send_sem, recv_sem, device):
    pltpu.make_async_remote_copy(
        src_ref=src,
        dst_ref=dst,
        send_sem=send_sem,
        recv_sem=recv_sem,
        device_id=device,
        device_id_type=MESH,
    ).start()


def landed(ref, sem):
    with jax.named_scope("wait"):
        pltpu.make_async_copy(ref, ref, sem).wait()


def minus_expm1(u):
    series = 1.0 + u * (1.0 / 8.0)
    for k in (7.0, 6.0, 5.0, 4.0, 3.0, 2.0):
        series = 1.0 + (u * (1.0 / k)) * series
    return jnp.where(u > -0.5, -u * series, 1.0 - jnp.exp(u))


def kernel(
    tokens,
    rec_shard,
    gate_shard,
    out_shard,
    up_shard,
    down_shard,
    mixer_gain_in,
    conv_taps_in,
    recur_map_in,
    input_map_in,
    decay_param_in,
    mlp_gain_in,
    result,
    mixer_gain,
    conv_taps,
    recur_map,
    input_map,
    decay_param,
    mlp_gain,
    w_rec,
    w_gate,
    w_out,
    w_up,
    w_d0,
    w_d1,
    down_raw,
    w_dn,
    tok_all,
    mid_all,
    normed,
    padded,
    gate_act,
    decay,
    drive,
    mixed,
    squared,
    first_sum,
    m_part,
    m_core,
    m_half_sent,
    m_half_got,
    m_full_sent,
    m_full_got,
    f_part,
    f_core,
    f_half_sent,
    f_half_got,
    f_full_sent,
    f_full_got,
    local_sem,
    w_sem,
    w_sent,
    ag_sem,
    ag_sent,
    m_sem,
    m_sent,
    f_sem,
    f_sent,
):
    rep, fs, tp = lax.axis_index("rep"), lax.axis_index("fs"), lax.axis_index("tp")
    z, x = lax.div(fs, 4), lax.rem(fs, 4)
    y, core = lax.div(tp, 2), lax.rem(tp, 2)
    other = 1 - core
    xp, xm, x2 = lax.rem(x + 1, 4), lax.rem(x + 3, 4), lax.rem(x + 2, 4)
    zp, zm, z2 = lax.rem(z + 1, 4), lax.rem(z + 3, 4), lax.rem(z + 2, 4)
    yp, ym, y2 = lax.rem(y + 1, 4), lax.rem(y + 3, 4), lax.rem(y + 2, 4)
    deep = rep * 4 + z
    deep_p, deep_m = lax.rem(deep + 1, 8), lax.rem(deep + 7, 8)
    x_up, x_down = (rep, z * 4 + xp, tp), (rep, z * 4 + xm, tp)
    z_up = (lax.div(deep_p, 4), zp * 4 + x, tp)
    z_down = (lax.div(deep_m, 4), zm * 4 + x, tp)
    y_up, y_down = (rep, fs, yp * 2 + core), (rep, fs, ym * 2 + core)
    partner = (rep, fs, y * 2 + other)

    places = (
        (tokens, tok_all.at[tp]),
        (rec_shard, w_rec.at[z * 4 + x]),
        (gate_shard, w_gate.at[z * 4 + x]),
        (out_shard, w_out.at[z * 4 + x]),
        (up_shard, w_up.at[z * 4 + x]),
        (down_shard, down_raw),
        (mixer_gain_in, mixer_gain),
        (conv_taps_in, conv_taps),
        (recur_map_in, recur_map),
        (input_map_in, input_map),
        (decay_param_in, decay_param),
        (mlp_gain_in, mlp_gain),
    )
    fills = [pltpu.make_async_copy(s, d, local_sem.at[k]) for k, (s, d) in enumerate(places)]
    for fill in fills:
        fill.start()
    barrier = pltpu.get_barrier_semaphore()
    with jax.named_scope("barrier"):
        for device in (x_up, x_down, z_up, z_down, y_up, y_down, partner):
            pl.semaphore_signal(barrier, inc=1, device_id=device, device_id_type=MESH)
        pl.semaphore_wait(barrier, 7)
    for fill in fills:
        fill.wait()

    def copies(k, w, recv, *moves):
        for (i, j, rows), device in moves:
            ref = w.at[i * 4 + j, rows]
            send(ref, ref, w_sent.at[k], w_sem.at[k, recv], device)

    weights = {"rec": (0, w_rec), "gate": (1, w_gate), "out": (2, w_out), "up": (3, w_up), "d0": (4, w_d0), "d1": (5, w_d1)}

    def pieces(w):
        h = w.shape[1] // 2
        q = h // 2
        return pl.ds(0, h), pl.ds(h, h), pl.ds(0, q), pl.ds(q, q), pl.ds(h, q), pl.ds(h + q, q)

    def w1(name):
        k, w = weights[name]
        a, b, _, _, _, _ = pieces(w)
        copies(k, w, 0, ((z, x, a), x_up), ((z, x, a), x_down), ((z, x, b), z_up), ((z, x, b), z_down))
        copies(k, w, 2, ((z, x, a), z_up), ((z, x, a), z_down), ((z, x, b), x_up), ((z, x, b), x_down))

    def w2(name):
        k, w = weights[name]
        a, b, at, ab, bt, bb = pieces(w)
        landed(w.at[pl.ds(0, 2)], w_sem.at[k, 0])
        copies(k, w, 1, ((z, xm, at), x_up), ((z, xp, ab), x_down), ((zm, x, bt), z_up), ((zp, x, bb), z_down))
        for n in (xm, xp):
            copies(k, w, 2, ((z, n, a), z_up), ((z, n, a), z_down))
        for n in (zm, zp):
            copies(k, w, 2, ((n, x, b), x_up), ((n, x, b), x_down))

    def w3(name):
        k, w = weights[name]
        a, b, _, _, _, _ = pieces(w)
        landed(w.at[0], w_sem.at[k, 1])
        copies(k, w, 4, ((z, x2, a), z_up), ((z, x2, a), z_down), ((z2, x, b), x_up), ((z2, x, b), x_down))

    def w4(name):
        k, w = weights[name]
        _, _, at, ab, bt, bb = pieces(w)
        landed(w.at[pl.ds(0, 6)], w_sem.at[k, 2])
        for n in (x, xm, xp):
            copies(k, w, 3, ((zm, n, at), z_up), ((zp, n, ab), z_down))
        for n in (z, zm, zp):
            copies(k, w, 3, ((n, xm, bt), x_up), ((n, xp, bb), x_down))

    def w6(name):
        k, w = weights[name]
        _, _, at, ab, bt, bb = pieces(w)
        landed(w.at[pl.ds(0, 2)], w_sem.at[k, 4])
        copies(k, w, 3, ((zm, x2, at), z_up), ((zp, x2, ab), z_down), ((z2, xm, bt), x_up), ((z2, xp, bb), x_down))

    def w5(name):
        k, w = weights[name]
        landed(w.at[pl.ds(0, 4)], w_sem.at[k, 3])

    def w_drain():
        for k, w in weights.values():
            landed(w.at[pl.ds(0, 15)], w_sent.at[k])

    jp, jm, j2 = yp * 2 + core, ym * 2 + core, y2 * 2 + core

    def ag(k, buf, first, count, sent):
        rows, top, bottom = pl.ds(first, count), pl.ds(first, count // 2), pl.ds(first + count // 2, count // 2)
        sem = lambda n: ag_sem.at[k, n]
        move = lambda index, recv, device: send(buf.at[index], buf.at[index], sent, sem(recv), device)

        def one():
            move((tp, rows), 0, y_up)
            move((tp, rows), 0, y_down)
            move((tp, rows), 2, partner)

        def two():
            landed(buf.at[pl.ds(0, 2), rows], sem(0))
            move((jm, top), 1, y_up)
            move((jp, bottom), 1, y_down)
            move((jm, rows), 2, partner)
            move((jp, rows), 2, partner)

        def three():
            landed(buf.at[0, rows], sem(1))
            move((j2, rows), 2, partner)

        def four():
            landed(buf.at[pl.ds(0, 4), rows], sem(2))

        return one, two, three, four

    top, bottom = pl.ds(0, H), pl.ds(H, H)
    leaving = (y2, yp, ym, y)

    def rs(k, part, from_core, half_sent, half_got, full_sent, full_got, sems, sent):
        sem = lambda n: sems.at[k, n]
        both = lambda n: part[k, core, n].astype(F32) + from_core[k, n].astype(F32)

        def first():
            send(part.at[k, other, 0], from_core.at[k, 0], sent.at[0], sem(0), partner)

        def rest():
            send(part.at[k, other, pl.ds(1, 3)], from_core.at[k, pl.ds(1, 3)], sent.at[0], sem(1), partner)

        def one():
            landed(from_core.at[k, 0], sem(0))
            half_sent[k] = both(0).astype(BF16)
            send(half_sent.at[k, top], half_got.at[k, top], sent.at[1], sem(1), y_up)
            send(half_sent.at[k, bottom], half_got.at[k, bottom], sent.at[1], sem(1), y_down)

        def two():
            landed(from_core.at[k], sem(1))
            up, down = both(1), both(2)
            got = half_got[k].astype(F32)
            full_sent[k, 0] = jnp.concatenate([up[:H] + got[:H], up[H:]], axis=0).astype(BF16)
            send(full_sent.at[k, 0], full_got.at[k, 0], sent.at[2], sem(2), y_up)
            full_sent[k, 1] = jnp.concatenate([down[:H], down[H:] + got[H:]], axis=0).astype(BF16)
            send(full_sent.at[k, 1], full_got.at[k, 1], sent.at[2], sem(2), y_down)

        def three():
            landed(full_got.at[k], sem(2))
            return both(3) + (full_got[k, 0].astype(F32) + full_got[k, 1].astype(F32))

        return first, one, two, three, rest

    def norm(buf, gain, first, count):
        step = count // 2

        def body(i, _):
            rows = pl.ds(pl.multiple_of(first + i * step, 32), step)
            total = jnp.zeros((step, CH), F32)
            for j in range(8):
                v = buf[j, rows, :].astype(F32)
                total = total + v * v
            inverse = lax.rsqrt(jnp.sum(total, axis=-1, keepdims=True) * (1.0 / D) + NORM_EPSILON)
            for j in range(8):
                v = buf[j, rows, :].astype(F32)
                normed[rows, CH * j : CH * (j + 1)] = (v * inverse * gain[:, CH * j : CH * (j + 1)]).astype(BF16)
            return 0

        lax.fori_loop(0, count // step, body, 0)

    def project(m):
        rows = pl.ds(m * 256, 256)
        lhs = normed[rows, :]
        branch = jnp.dot(lhs, w_rec[...].reshape(D, CH), preferred_element_type=F32)
        padded[pl.ds(m * 256 + 8, 256), :] = branch.astype(BF16).astype(F32)
        gate = jnp.dot(lhs, w_gate[...].reshape(D, CH), preferred_element_type=F32)
        gate_act[rows, :] = jax.nn.gelu(gate.astype(BF16).astype(F32), approximate=True)

    def gates(m, _):
        rows = pl.ds(pl.multiple_of(m * 128, 128), 128)
        window = padded[pl.ds(pl.multiple_of(m * 128, 128), 136), :]
        running = jnp.zeros((128, CH), F32)
        for k in range(4):
            running = running + window[5 + k : 133 + k] * conv_taps[k : k + 1, :].astype(F32)
        conv = running.astype(BF16)
        recur = jax.nn.sigmoid(jnp.dot(conv, recur_map[0], preferred_element_type=F32))
        enter = jax.nn.sigmoid(jnp.dot(conv, input_map[0], preferred_element_type=F32))
        p = -decay_param[...]
        softplus = jnp.maximum(p, 0.0) + jnp.log1p(jnp.exp(-jnp.abs(p)))
        log_decay = -GATE_SCALE * recur * softplus
        a = jnp.exp(log_decay)
        s = jnp.sqrt(minus_expm1(2.0 * log_decay)) * (enter * conv.astype(F32))
        for half in range(2):
            cols = slice(128 * half, 128 * (half + 1))
            decay[half, rows, :] = a[:, cols]
            drive[half, rows, :] = s[:, cols]
        return 0

    carries = [jnp.zeros((1, 128), F32)] * 2

    def scan(m):
        base = m * PART

        def body(k, carry):
            new = []
            for half in range(2):
                h, p = carry[half]
                at = pl.ds(base + k, SEGS, SEG)
                a = decay[half, at, :]
                h = a * h + drive[half, at, :]
                p = a * p
                drive[half, at, :] = h
                decay[half, at, :] = p
                new.append((h, p))
            return tuple(new)

        first = (jnp.zeros((SEGS, 128), F32), jnp.ones((SEGS, 128), F32))
        lax.fori_loop(0, SEG, body, (first, first), unroll=8)
        for half in range(2):
            cols = slice(128 * half, 128 * (half + 1))
            carry = carries[half]
            for n in range(SEGS):
                rows = slice(base + SEG * n, base + SEG * (n + 1))
                state = drive[half, rows, :] + decay[half, rows, :] * carry
                carry = state[SEG - 1 : SEG]
                mixed[rows, cols] = (state * gate_act[rows, cols]).astype(BF16)
            carries[half] = carry

    def out_product(c):
        lhs = mixed[pl.ds(c * R, R), :]

        def term(r, side):
            place = 4 * leaving[r] + 2 * side
            rhs = jnp.concatenate([w_out[place], w_out[place + 1]], axis=1)
            m_part[c, side, r] = jnp.dot(lhs, rhs, preferred_element_type=F32).astype(BF16)

        for r in range(4):
            term(r, other)
        mixer[c][0]()
        mixer[c][4]()
        for r in range(4):
            term(r, core)

    def lift(c):
        lhs = normed[pl.ds(c * R, R), :]
        for n in range(FF // 256):
            rhs = w_up[:, :, 256 * n : 256 * (n + 1)].reshape(D, 256)
            lifted = jnp.maximum(jnp.dot(lhs, rhs, preferred_element_type=F32), 0.0)
            squared[pl.ds(c * R, R), 256 * n : 256 * (n + 1)] = (lifted * lifted).astype(BF16)

    def low_lanes(shape):
        return lax.broadcasted_iota(jnp.int32, shape, 1) < 64

    def pack():
        step, odd = 128, lax.rem(x, 2)

        def body(i, _):
            upper = down_raw[pl.ds(pl.multiple_of(i * step + odd * (FF // 2), step), step), :].astype(F32)
            lower = down_raw[pl.ds(pl.multiple_of(i * step + (1 - odd) * (FF // 2), step), step), :].astype(F32)
            low = low_lanes((step, 128))
            rows = pl.ds(pl.multiple_of(i * step, step), step)
            w_d0[z * 4 + x, rows, :] = jnp.where(low, upper, pltpu.roll(lower, 64, 1)).astype(BF16)
            w_d1[z * 4 + x, rows, :] = jnp.where(low, pltpu.roll(upper, 64, 1), lower).astype(BF16)
            return 0

        lax.fori_loop(0, FF // 2 // step, body, 0)

    def unpack_rows(g, n, side, first):
        w, step = (w_d0, w_d1)[g], FF // 4
        low = low_lanes((128, 128))
        cols = pl.ds(pl.multiple_of(128 * side, 128), 128)
        for k in range(step // 128):
            left = w[4 * n + 2 * side, pl.ds(first + 128 * k, 128), :]
            right = w[4 * n + 2 * side + 1, pl.ds(first + 128 * k, 128), :]
            w_dn[g, n, pl.ds(first + 128 * k, 128), cols] = jnp.where(low, left, right)
            swapped = jnp.where(low, right, left).astype(F32)
            w_dn[g, n, pl.ds(first + FF // 2 + 128 * k, 128), cols] = pltpu.roll(swapped, 64, 1).astype(BF16)

    def unpack(g, late):
        pair = lax.div(x, 2)

        def body(i, _):
            if late:
                unpack_rows(g, i, 1 - pair, FF // 4)
            else:
                unpack_rows(g, i, pair, FF // 4)
            return 0

        lax.fori_loop(0, 4, body, 0)
        for n in (z2,) if late else (z, zm, zp):
            for side in range(2):
                unpack_rows(g, n, side, 0)

    def down_product(g, c, terms):
        k = g * CHUNKS + c
        lhs = squared[pl.ds(c * R, R), :]
        for r in terms:
            product = jnp.dot(lhs, w_dn[g, leaving[r]], preferred_element_type=F32).astype(BF16)
            f_part[k, 0, r] = product[:, :128]
            f_part[k, 1, r] = product[:, 128:]

    parts = [ag(n, tok_all, n * PART, PART, ag_sent.at[0]) for n in range(PARTS)]
    spread = [ag(PARTS + c, mid_all, c * R, R, ag_sent.at[1]) for c in range(CHUNKS)]
    m_bufs = (m_part, m_core, m_half_sent, m_half_got, m_full_sent, m_full_got, m_sem, m_sent)
    f_bufs = (f_part, f_core, f_half_sent, f_half_got, f_full_sent, f_full_got, f_sem, f_sent)
    mixer = [rs(c, *m_bufs) for c in range(CHUNKS)]
    mlp = [rs(k, *f_bufs) for k in range(2 * CHUNKS)]

    def middle(c):
        rows = pl.ds(c * R, R)
        total = mixer[c][3]()
        mid_all[tp, rows, :] = (tok_all[tp, rows, :].astype(F32) + total).astype(BF16)
        spread[c][0]()

    def feed(c):
        spread[c][3]()
        norm(mid_all, mlp_gain, c * R, R)
        lift(c)

    def finish(g, c):
        rows = pl.ds(c * R, R)
        total = mlp[g * CHUNKS + c][3]()
        if g == 0:
            first_sum[rows, :] = total
        else:
            early, low = first_sum[rows, :], low_lanes((R, 128))
            left = jnp.where(low, early, pltpu.roll(total, 64, 1))
            right = jnp.where(low, pltpu.roll(early, 64, 1), total)
            result[rows, :128] = (mid_all[tp, rows, :128].astype(F32) + left).astype(BF16)
            result[rows, 128:] = (mid_all[tp, rows, 128:].astype(F32) + right).astype(BF16)

    w_steps = {"w1": w1, "w2": w2, "w3": w3, "w4": w4, "w5": w5, "w6": w6}

    def part_start(m):
        if m == 0:
            padded[pl.ds(0, 8), :] = jnp.zeros((8, CH), F32)
            w5("rec")
            w5("gate")
        project(m)

    def part_end(m):
        lax.fori_loop(2 * m, 2 * m + 2, gates, 0)
        scan(m)

    m_steps = (
        out_product,
        lambda c: mixer[c][1](),
        lambda c: mixer[c][2](),
        middle,
        lambda c: spread[c][1](),
        lambda c: spread[c][2](),
        feed,
    )

    def f_step(stage, g, c):
        if stage == 0:
            down_product(g, c, (0, 1, 2, 3))
            mlp[g * CHUNKS + c][0]()
            mlp[g * CHUNKS + c][4]()
        elif stage == 5:
            for n in range(CHUNKS):
                down_product(g, n, (0,))
            for n in range(CHUNKS):
                mlp[g * CHUNKS + n][0]()
        elif stage == 4:
            down_product(g, c, (1, 2, 3))
            mlp[g * CHUNKS + c][4]()
        elif stage == 3:
            finish(g, c)
        else:
            mlp[g * CHUNKS + c][stage]()

    def do(*words):
        for word in words:
            with jax.named_scope(word):
                kind, digits = word[0], [int(d) for d in word[1:] if d.isdigit()]
                if kind == "w":
                    w_steps[word[:2]](word[3:])
                elif kind == "t":
                    parts[digits[1]][digits[0] - 1]()
                elif kind == "p":
                    pack()
                elif kind == "a":
                    norm(tok_all, mixer_gain, digits[0] * PART, PART)
                elif kind == "n":
                    part_start(*digits)
                elif kind == "g":
                    part_end(*digits)
                elif kind == "m":
                    m_steps[digits[0]](digits[1])
                elif kind == "u":
                    unpack(*digits)
                else:
                    f_step(*digits)

    do("w1_rec", "w1_gate", "t10", "t11", "t12", "w1_out", "p", "w2_rec", "w2_gate", "t20", "w2_out", "w3_rec", "w3_gate", "t21")
    do("w4_rec", "w4_gate", "w3_out", "t22", "w6_rec", "w6_gate", "t30", "w4_out", "t31", "t40", "a0", "w6_out", "w1_up", "w1_d0")
    do("t41", "a1", "n0", "t32", "g0", "w5_out", "m00", "n1", "m10", "g1", "w2_up", "m01", "t42", "a2", "n2", "m20", "m11", "g2")
    do("m02", "m03", "m12", "m13", "m30", "w3_up", "w2_d0", "m21", "m22", "m23", "w4_up", "m40", "m31", "w6_up", "w3_d0", "w1_d1")
    do("m32", "w4_d0", "m33", "m50", "m41", "w5_up", "m60", "m42", "w6_d0", "w2_d1", "m43", "m51", "u00", "m52", "m61", "m53")
    do("m62", "w3_d1", "w5_d0", "u01", "m63", "w4_d1", "f000", "f001", "f100", "w6_d1", "f002", "f101", "f003", "f102", "u10", "f103")
    do("f200", "f201", "w5_d1", "u11", "f510", "f410", "f202", "f110", "f111", "f411", "f112", "f113", "f203", "f412", "f413", "f300")
    do("f210", "f211", "f212", "f301", "f213", "f302", "f303", "f310", "f311", "f312", "f313")

    with jax.named_scope("drain"):
        w_drain()
        landed(tok_all.at[pl.ds(0, 7)], ag_sent.at[0])
        landed(mid_all.at[pl.ds(0, 7)], ag_sent.at[1])
        for bufs in (m_bufs, f_bufs):
            _, from_core, half_sent, _, full_sent, _, _, sent = bufs
            landed(from_core, sent.at[0])
            landed(half_sent, sent.at[1])
            landed(full_sent, sent.at[2])


def shards(
    tokens,
    mixer_gain,
    rec_weight,
    gate_weight,
    conv_taps,
    recur_map,
    input_map,
    decay_param,
    out_weight,
    mlp_gain,
    up_weight,
    down_weight,
):
    hbm = pl.BlockSpec(memory_space=pl.ANY)

    def sums(count, width):
        shapes = [(2, 4, R, width), (4, R, width), (R, width), (R, width), (2, R, width), (2, R, width)]
        return [pltpu.VMEM((count, *shape), BF16) for shape in shapes]

    return pl.pallas_call(
        kernel,
        out_shape=pltpu.VMEM((TOK, CH), BF16),
        in_specs=[hbm] * 12,
        out_specs=pl.BlockSpec(memory_space=pltpu.VMEM),
        scratch_shapes=[
            pltpu.VMEM((1, D), F32),
            pltpu.VMEM((4, CH), BF16),
            pltpu.VMEM((1, CH, CH), BF16),
            pltpu.VMEM((1, CH, CH), BF16),
            pltpu.VMEM((1, CH), F32),
            pltpu.VMEM((1, D), F32),
            pltpu.VMEM((16, D // 16, CH), BF16),
            pltpu.VMEM((16, D // 16, CH), BF16),
            pltpu.VMEM((16, CH, D // 16), BF16),
            pltpu.VMEM((16, D // 16, FF), BF16),
            pltpu.VMEM((16, FF // 2, D // 16), BF16),
            pltpu.VMEM((16, FF // 2, D // 16), BF16),
            pltpu.VMEM((FF, D // 16), BF16),
            pltpu.VMEM((2, 4, FF, CH), BF16),
            pltpu.VMEM((8, TOK, CH), BF16),
            pltpu.VMEM((8, TOK, CH), BF16),
            pltpu.VMEM((TOK, D), BF16),
            pltpu.VMEM((TOK + 8, CH), F32),
            pltpu.VMEM((TOK, CH), F32),
            pltpu.VMEM((2, TOK, 128), F32),
            pltpu.VMEM((2, TOK, 128), F32),
            pltpu.VMEM((TOK, CH), BF16),
            pltpu.VMEM((TOK, FF), BF16),
            pltpu.VMEM((TOK, 128), F32),
            *sums(CHUNKS, CH),
            *sums(2 * CHUNKS, CH // 2),
            pltpu.SemaphoreType.DMA((12,)),
            pltpu.SemaphoreType.DMA((6, 5)),
            pltpu.SemaphoreType.DMA((6,)),
            pltpu.SemaphoreType.DMA((PARTS + CHUNKS, 3)),
            pltpu.SemaphoreType.DMA((2,)),
            pltpu.SemaphoreType.DMA((CHUNKS, 3)),
            pltpu.SemaphoreType.DMA((3,)),
            pltpu.SemaphoreType.DMA((2 * CHUNKS, 3)),
            pltpu.SemaphoreType.DMA((3,)),
        ],
        compiler_params=pltpu.CompilerParams(
            collective_id=0, has_side_effects=True, vmem_limit_bytes=60 * 1024 * 1024
        ),
    )(
        tokens,
        rec_weight,
        gate_weight,
        out_weight,
        up_weight,
        down_weight,
        mixer_gain.reshape(1, D),
        conv_taps,
        recur_map,
        input_map,
        decay_param.reshape(1, CH),
        mlp_gain.reshape(1, D),
    )


def solution(mesh):
    placed = (
        P(("rep", "fs"), "tp"),
        P(),
        P("fs", "tp"),
        P("fs", "tp"),
        P(None, "tp"),
        P("tp", None, None),
        P("tp", None, None),
        P("tp"),
        P("tp", "fs"),
        P(),
        P("fs", "tp"),
        P("tp", "fs"),
    )
    return jax.shard_map(
        shards, mesh=mesh, in_specs=placed, out_specs=P(("rep", "fs"), "tp"), check_vma=False
    )
```

```python
import jax
import jax.numpy as jnp
from jax import lax
from jax.experimental import pallas as pl
from jax.experimental.pallas import tpu as pltpu
from jax.sharding import PartitionSpec as P

NORM_EPSILON = 1e-06
GATE_SCALE = 8.0
MESH = pl.DeviceIdType.MESH
F32 = jnp.float32
BF16 = jnp.bfloat16

TOK = 768
D = 2048
CH = 256
FF = 1024
CHUNKS = 4
PARTS = 3
PART = TOK // PARTS
R = TOK // CHUNKS
H = R // 2
SEGS = 16
SEG = PART // SEGS


def send(src, dst, send_sem, recv_sem, device):
    pltpu.make_async_remote_copy(
        src_ref=src,
        dst_ref=dst,
        send_sem=send_sem,
        recv_sem=recv_sem,
        device_id=device,
        device_id_type=MESH,
    ).start()


def landed(ref, sem):
    with jax.named_scope("wait"):
        pltpu.make_async_copy(ref, ref, sem).wait()


def minus_expm1(u):
    series = 1.0 + u * (1.0 / 8.0)
    for k in (7.0, 6.0, 5.0, 4.0, 3.0, 2.0):
        series = 1.0 + (u * (1.0 / k)) * series
    return jnp.where(u > -0.5, -u * series, 1.0 - jnp.exp(u))


def kernel(
    tokens,
    rec_shard,
    gate_shard,
    out_shard,
    up_shard,
    down_shard,
    mixer_gain_in,
    conv_taps_in,
    recur_map_in,
    input_map_in,
    decay_param_in,
    mlp_gain_in,
    result,
    mixer_gain,
    conv_taps,
    recur_map,
    input_map,
    decay_param,
    mlp_gain,
    w_rec,
    w_gate,
    w_out,
    w_up,
    w_d0,
    w_d1,
    down_raw,
    w_dn,
    tok_all,
    mid_all,
    normed,
    padded,
    gate_act,
    decay,
    drive,
    mixed,
    squared,
    first_sum,
    m_part,
    m_core,
    m_half_sent,
    m_half_got,
    m_full_sent,
    m_full_got,
    f_part,
    f_core,
    f_half_sent,
    f_half_got,
    f_full_sent,
    f_full_got,
    local_sem,
    w_sem,
    w_sent,
    ag_sem,
    ag_sent,
    m_sem,
    m_sent,
    f_sem,
    f_sent,
):
    rep, fs, tp = lax.axis_index("rep"), lax.axis_index("fs"), lax.axis_index("tp")
    z, x = lax.div(fs, 4), lax.rem(fs, 4)
    y, core = lax.div(tp, 2), lax.rem(tp, 2)
    other = 1 - core
    xp, xm, x2 = lax.rem(x + 1, 4), lax.rem(x + 3, 4), lax.rem(x + 2, 4)
    zp, zm, z2 = lax.rem(z + 1, 4), lax.rem(z + 3, 4), lax.rem(z + 2, 4)
    yp, ym, y2 = lax.rem(y + 1, 4), lax.rem(y + 3, 4), lax.rem(y + 2, 4)
    deep = rep * 4 + z
    deep_p, deep_m = lax.rem(deep + 1, 8), lax.rem(deep + 7, 8)
    x_up, x_down = (rep, z * 4 + xp, tp), (rep, z * 4 + xm, tp)
    z_up = (lax.div(deep_p, 4), zp * 4 + x, tp)
    z_down = (lax.div(deep_m, 4), zm * 4 + x, tp)
    y_up, y_down = (rep, fs, yp * 2 + core), (rep, fs, ym * 2 + core)
    partner = (rep, fs, y * 2 + other)

    places = (
        (tokens, tok_all.at[tp]),
        (rec_shard, w_rec.at[z * 4 + x]),
        (gate_shard, w_gate.at[z * 4 + x]),
        (out_shard, w_out.at[z * 4 + x]),
        (up_shard, w_up.at[z * 4 + x]),
        (down_shard, down_raw),
        (mixer_gain_in, mixer_gain),
        (conv_taps_in, conv_taps),
        (recur_map_in, recur_map),
        (input_map_in, input_map),
        (decay_param_in, decay_param),
        (mlp_gain_in, mlp_gain),
    )
    fills = [pltpu.make_async_copy(s, d, local_sem.at[k]) for k, (s, d) in enumerate(places)]
    for fill in fills:
        fill.start()
    barrier = pltpu.get_barrier_semaphore()
    with jax.named_scope("barrier"):
        for device in (x_up, x_down, z_up, z_down, y_up, y_down, partner):
            pl.semaphore_signal(barrier, inc=1, device_id=device, device_id_type=MESH)
        pl.semaphore_wait(barrier, 7)
    for fill in fills:
        fill.wait()

    def copies(k, w, recv, *moves):
        for (i, j, rows), device in moves:
            ref = w.at[i * 4 + j, rows]
            send(ref, ref, w_sent.at[k], w_sem.at[k, recv], device)

    weights = {"rec": (0, w_rec), "gate": (1, w_gate), "out": (2, w_out), "up": (3, w_up), "d0": (4, w_d0), "d1": (5, w_d1)}

    def pieces(w):
        h = w.shape[1] // 2
        q = h // 2
        return pl.ds(0, h), pl.ds(h, h), pl.ds(0, q), pl.ds(q, q), pl.ds(h, q), pl.ds(h + q, q)

    def w1(name):
        k, w = weights[name]
        a, b, _, _, _, _ = pieces(w)
        copies(k, w, 0, ((z, x, a), x_up), ((z, x, a), x_down), ((z, x, b), z_up), ((z, x, b), z_down))
        copies(k, w, 2, ((z, x, a), z_up), ((z, x, a), z_down), ((z, x, b), x_up), ((z, x, b), x_down))

    def w2(name):
        k, w = weights[name]
        a, b, at, ab, bt, bb = pieces(w)
        landed(w.at[pl.ds(0, 2)], w_sem.at[k, 0])
        copies(k, w, 1, ((z, xm, at), x_up), ((z, xp, ab), x_down), ((zm, x, bt), z_up), ((zp, x, bb), z_down))
        for n in (xm, xp):
            copies(k, w, 2, ((z, n, a), z_up), ((z, n, a), z_down))
        for n in (zm, zp):
            copies(k, w, 2, ((n, x, b), x_up), ((n, x, b), x_down))

    def w3(name):
        k, w = weights[name]
        a, b, _, _, _, _ = pieces(w)
        landed(w.at[0], w_sem.at[k, 1])
        copies(k, w, 4, ((z, x2, a), z_up), ((z, x2, a), z_down), ((z2, x, b), x_up), ((z2, x, b), x_down))

    def w4(name):
        k, w = weights[name]
        _, _, at, ab, bt, bb = pieces(w)
        landed(w.at[pl.ds(0, 6)], w_sem.at[k, 2])
        for n in (x, xm, xp):
            copies(k, w, 3, ((zm, n, at), z_up), ((zp, n, ab), z_down))
        for n in (z, zm, zp):
            copies(k, w, 3, ((n, xm, bt), x_up), ((n, xp, bb), x_down))

    def w6(name):
        k, w = weights[name]
        _, _, at, ab, bt, bb = pieces(w)
        landed(w.at[pl.ds(0, 2)], w_sem.at[k, 4])
        copies(k, w, 3, ((zm, x2, at), z_up), ((zp, x2, ab), z_down), ((z2, xm, bt), x_up), ((z2, xp, bb), x_down))

    def w5(name):
        k, w = weights[name]
        landed(w.at[pl.ds(0, 4)], w_sem.at[k, 3])

    def w_drain():
        for k, w in weights.values():
            landed(w.at[pl.ds(0, 15)], w_sent.at[k])

    jp, jm, j2 = yp * 2 + core, ym * 2 + core, y2 * 2 + core

    def ag(k, buf, first, count, sent):
        rows, top, bottom = pl.ds(first, count), pl.ds(first, count // 2), pl.ds(first + count // 2, count // 2)
        sem = lambda n: ag_sem.at[k, n]
        move = lambda index, recv, device: send(buf.at[index], buf.at[index], sent, sem(recv), device)

        def one():
            move((tp, rows), 0, y_up)
            move((tp, rows), 0, y_down)
            move((tp, rows), 2, partner)

        def two():
            landed(buf.at[pl.ds(0, 2), rows], sem(0))
            move((jm, top), 1, y_up)
            move((jp, bottom), 1, y_down)
            move((jm, rows), 2, partner)
            move((jp, rows), 2, partner)

        def three():
            landed(buf.at[0, rows], sem(1))
            move((j2, rows), 2, partner)

        def four():
            landed(buf.at[pl.ds(0, 4), rows], sem(2))

        return one, two, three, four

    top, bottom = pl.ds(0, H), pl.ds(H, H)
    leaving = (y2, yp, ym, y)

    def rs(k, part, from_core, half_sent, half_got, full_sent, full_got, sems, sent):
        sem = lambda n: sems.at[k, n]
        both = lambda n: part[k, core, n].astype(F32) + from_core[k, n].astype(F32)

        def first():
            send(part.at[k, other, 0], from_core.at[k, 0], sent.at[0], sem(0), partner)

        def rest():
            send(part.at[k, other, pl.ds(1, 3)], from_core.at[k, pl.ds(1, 3)], sent.at[0], sem(1), partner)

        def one():
            landed(from_core.at[k, 0], sem(0))
            half_sent[k] = both(0).astype(BF16)
            send(half_sent.at[k, top], half_got.at[k, top], sent.at[1], sem(1), y_up)
            send(half_sent.at[k, bottom], half_got.at[k, bottom], sent.at[1], sem(1), y_down)

        def two():
            landed(from_core.at[k], sem(1))
            up, down = both(1), both(2)
            got = half_got[k].astype(F32)
            full_sent[k, 0] = jnp.concatenate([up[:H] + got[:H], up[H:]], axis=0).astype(BF16)
            send(full_sent.at[k, 0], full_got.at[k, 0], sent.at[2], sem(2), y_up)
            full_sent[k, 1] = jnp.concatenate([down[:H], down[H:] + got[H:]], axis=0).astype(BF16)
            send(full_sent.at[k, 1], full_got.at[k, 1], sent.at[2], sem(2), y_down)

        def three():
            landed(full_got.at[k], sem(2))
            return both(3) + (full_got[k, 0].astype(F32) + full_got[k, 1].astype(F32))

        return first, one, two, three, rest

    def norm(buf, gain, first, count):
        step = count // 2

        def body(i, _):
            rows = pl.ds(pl.multiple_of(first + i * step, 32), step)
            total = jnp.zeros((step, CH), F32)
            for j in range(8):
                v = buf[j, rows, :].astype(F32)
                total = total + v * v
            inverse = lax.rsqrt(jnp.sum(total, axis=-1, keepdims=True) * (1.0 / D) + NORM_EPSILON)
            for j in range(8):
                v = buf[j, rows, :].astype(F32)
                normed[rows, CH * j : CH * (j + 1)] = (v * inverse * gain[:, CH * j : CH * (j + 1)]).astype(BF16)
            return 0

        lax.fori_loop(0, count // step, body, 0)

    def project(m):
        rows = pl.ds(m * 256, 256)
        lhs = normed[rows, :]
        branch = jnp.dot(lhs, w_rec[...].reshape(D, CH), preferred_element_type=F32)
        padded[pl.ds(m * 256 + 8, 256), :] = branch.astype(BF16).astype(F32)
        gate = jnp.dot(lhs, w_gate[...].reshape(D, CH), preferred_element_type=F32)
        gate_act[rows, :] = jax.nn.gelu(gate.astype(BF16).astype(F32), approximate=True)

    def gates(m, _):
        rows = pl.ds(pl.multiple_of(m * 128, 128), 128)
        window = padded[pl.ds(pl.multiple_of(m * 128, 128), 136), :]
        running = jnp.zeros((128, CH), F32)
        for k in range(4):
            running = running + window[5 + k : 133 + k] * conv_taps[k : k + 1, :].astype(F32)
        conv = running.astype(BF16)
        recur = jax.nn.sigmoid(jnp.dot(conv, recur_map[0], preferred_element_type=F32))
        enter = jax.nn.sigmoid(jnp.dot(conv, input_map[0], preferred_element_type=F32))
        p = -decay_param[...]
        softplus = jnp.maximum(p, 0.0) + jnp.log1p(jnp.exp(-jnp.abs(p)))
        log_decay = -GATE_SCALE * recur * softplus
        a = jnp.exp(log_decay)
        s = jnp.sqrt(minus_expm1(2.0 * log_decay)) * (enter * conv.astype(F32))
        for half in range(2):
            cols = slice(128 * half, 128 * (half + 1))
            decay[half, rows, :] = a[:, cols]
            drive[half, rows, :] = s[:, cols]
        return 0

    carries = [jnp.zeros((1, 128), F32)] * 2

    def scan(m):
        base = m * PART

        def body(k, carry):
            new = []
            for half in range(2):
                h, p = carry[half]
                at = pl.ds(base + k, SEGS, SEG)
                a = decay[half, at, :]
                h = a * h + drive[half, at, :]
                p = a * p
                drive[half, at, :] = h
                decay[half, at, :] = p
                new.append((h, p))
            return tuple(new)

        first = (jnp.zeros((SEGS, 128), F32), jnp.ones((SEGS, 128), F32))
        lax.fori_loop(0, SEG, body, (first, first), unroll=8)
        for half in range(2):
            cols = slice(128 * half, 128 * (half + 1))
            carry = carries[half]
            for n in range(SEGS):
                rows = slice(base + SEG * n, base + SEG * (n + 1))
                state = drive[half, rows, :] + decay[half, rows, :] * carry
                carry = state[SEG - 1 : SEG]
                mixed[rows, cols] = (state * gate_act[rows, cols]).astype(BF16)
            carries[half] = carry

    def out_product(c):
        lhs = mixed[pl.ds(c * R, R), :]

        def term(r, side):
            place = 4 * leaving[r] + 2 * side
            rhs = jnp.concatenate([w_out[place], w_out[place + 1]], axis=1)
            m_part[c, side, r] = jnp.dot(lhs, rhs, preferred_element_type=F32).astype(BF16)

        for r in range(4):
            term(r, other)
        mixer[c][0]()
        mixer[c][4]()
        for r in range(4):
            term(r, core)

    def lift(c):
        lhs = normed[pl.ds(c * R, R), :]
        for n in range(FF // 256):
            rhs = w_up[:, :, 256 * n : 256 * (n + 1)].reshape(D, 256)
            lifted = jnp.maximum(jnp.dot(lhs, rhs, preferred_element_type=F32), 0.0)
            squared[pl.ds(c * R, R), 256 * n : 256 * (n + 1)] = (lifted * lifted).astype(BF16)

    def low_lanes(shape):
        return lax.broadcasted_iota(jnp.int32, shape, 1) < 64

    def pack():
        step, odd = 128, lax.rem(x, 2)

        def body(i, _):
            upper = down_raw[pl.ds(pl.multiple_of(i * step + odd * (FF // 2), step), step), :].astype(F32)
            lower = down_raw[pl.ds(pl.multiple_of(i * step + (1 - odd) * (FF // 2), step), step), :].astype(F32)
            low = low_lanes((step, 128))
            rows = pl.ds(pl.multiple_of(i * step, step), step)
            w_d0[z * 4 + x, rows, :] = jnp.where(low, upper, pltpu.roll(lower, 64, 1)).astype(BF16)
            w_d1[z * 4 + x, rows, :] = jnp.where(low, pltpu.roll(upper, 64, 1), lower).astype(BF16)
            return 0

        lax.fori_loop(0, FF // 2 // step, body, 0)

    def unpack_rows(g, n, side, first):
        w, step = (w_d0, w_d1)[g], FF // 4
        low = low_lanes((128, 128))
        cols = pl.ds(pl.multiple_of(128 * side, 128), 128)
        for k in range(step // 128):
            left = w[4 * n + 2 * side, pl.ds(first + 128 * k, 128), :]
            right = w[4 * n + 2 * side + 1, pl.ds(first + 128 * k, 128), :]
            w_dn[g, n, pl.ds(first + 128 * k, 128), cols] = jnp.where(low, left, right)
            swapped = jnp.where(low, right, left).astype(F32)
            w_dn[g, n, pl.ds(first + FF // 2 + 128 * k, 128), cols] = pltpu.roll(swapped, 64, 1).astype(BF16)

    def unpack(g, late):
        pair = lax.div(x, 2)

        def body(i, _):
            if late:
                unpack_rows(g, i, 1 - pair, FF // 4)
            else:
                unpack_rows(g, i, pair, FF // 4)
            return 0

        lax.fori_loop(0, 4, body, 0)
        for n in (z2,) if late else (z, zm, zp):
            for side in range(2):
                unpack_rows(g, n, side, 0)

    def down_product(g, c, terms):
        k = g * CHUNKS + c
        lhs = squared[pl.ds(c * R, R), :]
        for r in terms:
            product = jnp.dot(lhs, w_dn[g, leaving[r]], preferred_element_type=F32).astype(BF16)
            f_part[k, 0, r] = product[:, :128]
            f_part[k, 1, r] = product[:, 128:]

    parts = [ag(n, tok_all, n * PART, PART, ag_sent.at[0]) for n in range(PARTS)]
    spread = [ag(PARTS + c, mid_all, c * R, R, ag_sent.at[1]) for c in range(CHUNKS)]
    m_bufs = (m_part, m_core, m_half_sent, m_half_got, m_full_sent, m_full_got, m_sem, m_sent)
    f_bufs = (f_part, f_core, f_half_sent, f_half_got, f_full_sent, f_full_got, f_sem, f_sent)
    mixer = [rs(c, *m_bufs) for c in range(CHUNKS)]
    mlp = [rs(k, *f_bufs) for k in range(2 * CHUNKS)]

    def middle(c):
        rows = pl.ds(c * R, R)
        total = mixer[c][3]()
        mid_all[tp, rows, :] = (tok_all[tp, rows, :].astype(F32) + total).astype(BF16)
        spread[c][0]()

    def feed(c):
        spread[c][3]()
        norm(mid_all, mlp_gain, c * R, R)
        lift(c)

    def finish(g, c):
        rows = pl.ds(c * R, R)
        total = mlp[g * CHUNKS + c][3]()
        if g == 0:
            first_sum[rows, :] = total
        else:
            early, low = first_sum[rows, :], low_lanes((R, 128))
            left = jnp.where(low, early, pltpu.roll(total, 64, 1))
            right = jnp.where(low, pltpu.roll(early, 64, 1), total)
            result[rows, :128] = (mid_all[tp, rows, :128].astype(F32) + left).astype(BF16)
            result[rows, 128:] = (mid_all[tp, rows, 128:].astype(F32) + right).astype(BF16)

    w_steps = {"w1": w1, "w2": w2, "w3": w3, "w4": w4, "w5": w5, "w6": w6}

    def part_start(m):
        if m == 0:
            padded[pl.ds(0, 8), :] = jnp.zeros((8, CH), F32)
            w5("rec")
            w5("gate")
        project(m)

    def part_end(m):
        lax.fori_loop(2 * m, 2 * m + 2, gates, 0)
        scan(m)

    m_steps = (
        out_product,
        lambda c: mixer[c][1](),
        lambda c: mixer[c][2](),
        middle,
        lambda c: spread[c][1](),
        lambda c: spread[c][2](),
        feed,
    )

    def f_step(stage, g, c):
        if stage == 0:
            down_product(g, c, (0, 1, 2, 3))
            mlp[g * CHUNKS + c][0]()
            mlp[g * CHUNKS + c][4]()
        elif stage == 5:
            for n in range(CHUNKS):
                down_product(g, n, (0,))
            for n in range(CHUNKS):
                mlp[g * CHUNKS + n][0]()
        elif stage == 4:
            down_product(g, c, (1, 2, 3))
            mlp[g * CHUNKS + c][4]()
        elif stage == 3:
            finish(g, c)
        else:
            mlp[g * CHUNKS + c][stage]()

    def do(*words):
        for word in words:
            with jax.named_scope(word):
                kind, digits = word[0], [int(d) for d in word[1:] if d.isdigit()]
                if kind == "w":
                    w_steps[word[:2]](word[3:])
                elif kind == "t":
                    parts[digits[1]][digits[0] - 1]()
                elif kind == "p":
                    pack()
                elif kind == "a":
                    norm(tok_all, mixer_gain, digits[0] * PART, PART)
                elif kind == "n":
                    part_start(*digits)
                elif kind == "g":
                    part_end(*digits)
                elif kind == "m":
                    m_steps[digits[0]](digits[1])
                elif kind == "u":
                    unpack(*digits)
                else:
                    f_step(*digits)

    do("w1_rec", "w1_gate", "t10", "t11", "t12", "w1_out", "p", "w2_rec", "w2_gate", "t20", "w2_out", "w3_rec", "w3_gate", "t21")
    do("w4_rec", "w4_gate", "w3_out", "t22", "w6_rec", "w6_gate", "t30", "w4_out", "t31", "t40", "a0", "w6_out", "w1_up", "w1_d0")
    do("t41", "a1", "n0", "t32", "g0", "w5_out", "m00", "n1", "m10", "g1", "w2_up", "m01", "t42", "a2", "n2", "m20", "m11", "g2")
    do("m02", "m03", "m12", "m13", "m30", "w3_up", "w2_d0", "m21", "m22", "m23", "w4_up", "m40", "m31", "w6_up", "w3_d0", "w1_d1")
    do("m32", "w4_d0", "m33", "m50", "m41", "w5_up", "m60", "m42", "w6_d0", "w2_d1", "m43", "m51", "u00", "m52", "m61", "m53")
    do("m62", "w3_d1", "w5_d0", "u01", "m63", "w4_d1", "f000", "f001", "f100", "w6_d1", "f002", "f101", "f003", "f102", "u10", "f103")
    do("f200", "f201", "w5_d1", "u11", "f510", "f410", "f202", "f110", "f111", "f411", "f112", "f113", "f203", "f412", "f413", "f300")
    do("f210", "f211", "f212", "f301", "f213", "f302", "f303", "f310", "f311", "f312", "f313")

    with jax.named_scope("drain"):
        w_drain()
        landed(tok_all.at[pl.ds(0, 7)], ag_sent.at[0])
        landed(mid_all.at[pl.ds(0, 7)], ag_sent.at[1])
        for bufs in (m_bufs, f_bufs):
            _, from_core, half_sent, _, full_sent, _, _, sent = bufs
            landed(from_core, sent.at[0])
            landed(half_sent, sent.at[1])
            landed(full_sent, sent.at[2])


def shards(
    tokens,
    mixer_gain,
    rec_weight,
    gate_weight,
    conv_taps,
    recur_map,
    input_map,
    decay_param,
    out_weight,
    mlp_gain,
    up_weight,
    down_weight,
):
    hbm = pl.BlockSpec(memory_space=pl.ANY)

    def sums(count, width):
        shapes = [(2, 4, R, width), (4, R, width), (R, width), (R, width), (2, R, width), (2, R, width)]
        return [pltpu.VMEM((count, *shape), BF16) for shape in shapes]

    return pl.pallas_call(
        kernel,
        out_shape=pltpu.VMEM((TOK, CH), BF16),
        in_specs=[hbm] * 12,
        out_specs=pl.BlockSpec(memory_space=pltpu.VMEM),
        scratch_shapes=[
            pltpu.VMEM((1, D), F32),
            pltpu.VMEM((4, CH), BF16),
            pltpu.VMEM((1, CH, CH), BF16),
            pltpu.VMEM((1, CH, CH), BF16),
            pltpu.VMEM((1, CH), F32),
            pltpu.VMEM((1, D), F32),
            pltpu.VMEM((16, D // 16, CH), BF16),
            pltpu.VMEM((16, D // 16, CH), BF16),
            pltpu.VMEM((16, CH, D // 16), BF16),
            pltpu.VMEM((16, D // 16, FF), BF16),
            pltpu.VMEM((16, FF // 2, D // 16), BF16),
            pltpu.VMEM((16, FF // 2, D // 16), BF16),
            pltpu.VMEM((FF, D // 16), BF16),
            pltpu.VMEM((2, 4, FF, CH), BF16),
            pltpu.VMEM((8, TOK, CH), BF16),
            pltpu.VMEM((8, TOK, CH), BF16),
            pltpu.VMEM((TOK, D), BF16),
            pltpu.VMEM((TOK + 8, CH), F32),
            pltpu.VMEM((TOK, CH), F32),
            pltpu.VMEM((2, TOK + SEG, 128), F32),
            pltpu.VMEM((2, TOK + SEG, 128), F32),
            pltpu.VMEM((TOK, CH), BF16),
            pltpu.VMEM((TOK, FF), BF16),
            pltpu.VMEM((TOK, 128), F32),
            *sums(CHUNKS, CH),
            *sums(2 * CHUNKS, CH // 2),
            pltpu.SemaphoreType.DMA((12,)),
            pltpu.SemaphoreType.DMA((6, 5)),
            pltpu.SemaphoreType.DMA((6,)),
            pltpu.SemaphoreType.DMA((PARTS + CHUNKS, 3)),
            pltpu.SemaphoreType.DMA((2,)),
            pltpu.SemaphoreType.DMA((CHUNKS, 3)),
            pltpu.SemaphoreType.DMA((3,)),
            pltpu.SemaphoreType.DMA((2 * CHUNKS, 3)),
            pltpu.SemaphoreType.DMA((3,)),
        ],
        compiler_params=pltpu.CompilerParams(
            collective_id=0, has_side_effects=True, vmem_limit_bytes=60 * 1024 * 1024
        ),
    )(
        tokens,
        rec_weight,
        gate_weight,
        out_weight,
        up_weight,
        down_weight,
        mixer_gain.reshape(1, D),
        conv_taps,
        recur_map,
        input_map,
        decay_param.reshape(1, CH),
        mlp_gain.reshape(1, D),
    )


def solution(mesh):
    placed = (
        P(("rep", "fs"), "tp"),
        P(),
        P("fs", "tp"),
        P("fs", "tp"),
        P(None, "tp"),
        P("tp", None, None),
        P("tp", None, None),
        P("tp"),
        P("tp", "fs"),
        P(),
        P("fs", "tp"),
        P("tp", "fs"),
    )
    return jax.shard_map(
        shards, mesh=mesh, in_specs=placed, out_specs=P(("rep", "fs"), "tp"), check_vma=False
    )
```
